128 devices in a mesh: rep: 2 (over z_hi), fs: 32 (over z_lo, y, x), tp: 2 (over core).
Axes of the slice: x: 4, y: 4, z: 4 (z_hi: 2, z_lo: 2; z = z_hi * 2 + z_lo), core: 2. Of those that a mesh axis runs over, the one named last changes fastest.
Arguments:
- tokens: bfloat16 [65536, 2048], P(('rep', 'fs', 'tp')), may hold values from -6 to 6
- pre_gain: bfloat16 [2048], replicated, may hold values from 0.099609375 to 1.8984375
- gate_weight: bfloat16 [2048, 2816], P('fs', 'tp'), may hold values from -0.125 to 0.125
- value_weight: bfloat16 [2048, 2816], P('fs', 'tp'), may hold values from -0.125 to 0.125
- down_weight: bfloat16 [2816, 2048], P('tp', 'fs'), may hold values from -0.109375 to 0.109375
- post_gain: bfloat16 [2048], replicated, may hold values from 0.099609375 to 1.8984375
Outputs:
- updated: bfloat16 [65536, 2048], P(('rep', 'fs', 'tp'))
The draws below stay inside these ranges and needn't reach their ends.
All inputs are finite; a program needn't handle non-finite values.
Results may differ from the reference program's by a relative error of at most 0.0055.
Values may be sent and summed in bfloat16 or wider, within the bound.
A program may use at most 128 MiB of HBM per device.

```python
import jax
import jax.numpy as jnp
from jax import lax

D = 2048
FF = 2816
TOK_DEV = 512
TOKENS = 65536
N_REP = 2
N_FS = 32
N_TP = 2


def block_levels(own_key, dims, cuts, low, largest):
    def one(axis_at, shards_of):
        draws = jax.random.uniform(jax.random.fold_in(jax.random.fold_in(own_key, 6), axis_at), (shards_of,), jnp.float32, low / len(cuts), largest / len(cuts))
        return jnp.repeat(jnp.exp(draws), dims[axis_at] // shards_of).reshape((-1,) + (1,) * (len(dims) - axis_at - 1))

    level = one(*cuts[0])
    for cut in cuts[1:]:
        level = level * one(*cut)
    return level


def centred(own_key, extent, scale, limit, shards=(), held_as=jnp.bfloat16):
    entries = jax.random.normal(own_key, extent, jnp.float32) * scale
    if len(shards) > 0:
        entries = block_levels(own_key, extent, shards, -0.22, 0.18) * entries
    return jnp.clip(entries, min=-limit, max=limit).astype(held_as)


def setup_inputs(seed: int = 0) -> dict:
    key_list = jax.random.split(jax.random.key(seed), 7)
    return {
        "tokens": centred(key_list[0], (TOKENS, D), 1.0, 6.0, ((0, 128),)),
        "pre_gain": jnp.clip(1.0 + 0.18 * jax.random.normal(key_list[1], (D,), jnp.float32), 0.099609375, 1.8984375).astype(jnp.bfloat16),
        "gate_weight": centred(key_list[2], (D, FF), D ** -0.5, 0.125, ((0, 32), (1, 2))),
        "value_weight": centred(key_list[3], (D, FF), D ** -0.5, 0.125, ((0, 32), (1, 2))),
        "down_weight": centred(key_list[4], (FF, D), FF ** -0.5, 0.109375, ((0, 2), (1, 32))),
        "post_gain": jnp.clip(1.0 + 0.18 * jax.random.normal(key_list[5], (D,), jnp.float32), 0.099609375, 1.8984375).astype(jnp.bfloat16),
    }


eps_norm = 1e-06

def rms_rows(values_in, gain):
    floats = values_in.astype(jnp.float32)
    scaled = floats * lax.rsqrt(lax.optimization_barrier(jnp.mean(floats * floats, -1, keepdims=True)) + eps_norm)
    return scaled * gain.astype(jnp.float32)

def reference(tokens, pre_gain, gate_weight, value_weight, down_weight, post_gain):
    group_size = TOK_DEV * N_TP
    block_width = FF // N_TP
    grouped = tokens.reshape(N_REP * N_FS, group_size, D)

    def one_group(block_rows):
        normed = rms_rows(block_rows, pre_gain).astype(jnp.bfloat16)
        gate_proj = jnp.dot(normed, gate_weight, preferred_element_type=jnp.float32)
        value_proj = jnp.dot(normed, value_weight, preferred_element_type=jnp.float32)
        hidden = (jax.nn.silu(gate_proj) * value_proj).astype(jnp.bfloat16)
        total = jnp.zeros((group_size, D), jnp.float32)
        for block_index in range(N_TP):
            lower = block_index * block_width
            partial_term = jnp.dot(hidden[:, lower:lower + block_width], down_weight[lower:lower + block_width], preferred_element_type=jnp.float32).astype(jnp.bfloat16)
            total = total + lax.optimization_barrier(partial_term).astype(jnp.float32)
        branch = total.astype(jnp.bfloat16)
        return (block_rows.astype(jnp.float32) + 0.5 * rms_rows(branch, post_gain)).astype(jnp.bfloat16)
    return lax.map(one_group, grouped).reshape(TOKENS, D)
```

```python
import jax
import jax.numpy as jnp
from jax import lax
from jax.experimental import pallas as pl
from jax.experimental.pallas import tpu as pltpu
from jax.sharding import PartitionSpec as P

D, F, Q, TOK = 2048, 1408, 704, 512
SENT = 2048
EPS = 1e-06
F32, BF16 = jnp.float32, jnp.bfloat16


class Copy:
    def __init__(self, src, dst, here, send_sem, recv_sem, to):
        make = pltpu.make_async_remote_copy
        kind = dict(device_id=to, device_id_type=pl.DeviceIdType.MESH)
        self.out = make(src_ref=src, dst_ref=dst, send_sem=send_sem, recv_sem=recv_sem, **kind)
        self.into = make(src_ref=here, dst_ref=here, send_sem=send_sem, recv_sem=recv_sem, **kind)

    def start(self):
        self.out.start()

    def arrived(self):
        self.into.wait_recv()

    def left(self):
        self.out.wait_send()


def ring_copies(block, half, to_a, to_b, send, recv):
    c = []
    for way in (1, -1):
        c.append((block(0, 0), block(-way, 0), to_a[way]))
    for way, h in ((1, 0), (-1, 1)):
        c.append((half(-way, 0, h), half(2, 0, h), to_a[way]))
    for way in (1, -1):
        for oa in (0, -1, 1, 2):
            c.append((block(oa, 0), block(oa, -way), to_b[way]))
    for way, h in ((1, 0), (-1, 1)):
        for oa in (0, -1, 1, 2):
            c.append((half(oa, -way, h), half(oa, 2, h), to_b[way]))
    return [Copy(ref, ref, here, send.at[i], recv.at[i], to) for i, (ref, here, to) in enumerate(c)]


def kernel(tok_in, pre_ref, gate_in, value_in, down_in, post_ref, out_ref, tok, wg, wv, wd, dd, dz, w, d, t, acc, hid, ps,
           pr, rp, zs, zr, own, os_, or_, load, ag_s, ag_r, zw_s, zw_r, tk_s, tk_r, p2_s, p2_r):
    rep, fs, core = lax.axis_index("rep"), lax.axis_index("fs"), lax.axis_index("tp")
    zlo, y, x = fs // 16, (fs // 4) % 4, fs % 4
    z = rep * 2 + zlo

    def device(dz_=0, dy=0, dx=0, other=False):
        zz, yy, xx = (z + dz_ + 4) % 4, (y + dy + 4) % 4, (x + dx + 4) % 4
        return {"rep": zz // 2, "fs": (zz % 2) * 16 + yy * 4 + xx, "tp": 1 - core if other else core}

    to_x = {1: device(dx=1), -1: device(dx=-1)}
    to_y = {1: device(dy=1), -1: device(dy=-1)}
    to_z = {1: device(dz_=1), -1: device(dz_=-1)}
    partner = device(other=True)

    loads = [
        pltpu.make_async_copy(gate_in, wg, load.at[0]),
        pltpu.make_async_copy(value_in, wv, load.at[1]),
        pltpu.make_async_copy(down_in, wd.at[0:64], load.at[2]),
        pltpu.make_async_copy(down_in, wd.at[64:128], load.at[3]),
        pltpu.make_async_copy(tok_in, tok, load.at[4]),
    ]
    for c in loads:
        c.start()

    barrier = pltpu.get_barrier_semaphore()
    for peer in (*to_x.values(), *to_y.values(), *to_z.values(), partner):
        pl.semaphore_signal(barrier, inc=1, device_id=peer, device_id_type=pl.DeviceIdType.MESH)

    lanes = lax.broadcasted_iota(jnp.int32, (64, 128), 1)
    low = lanes < 64
    swap = lambda v: pltpu.roll(v, 64, 1)

    loads[0].wait()
    loads[1].wait()
    place = (y * 4 + x) * 64
    for q in (0, 1):
        at = pl.multiple_of(place + (zlo + q) % 2 * (2048 - place), 64)
        g5, v5 = wg[:, 640:768].astype(F32), wv[:, 640:768].astype(F32)
        first = 768 * q
        w[pl.ds(at, 64), 0:640] = wg[:, first:first + 640]
        w[pl.ds(at, 64), 640:1280] = wv[:, first:first + 640]
        mixed = jnp.where(low, g5, swap(v5)) if q == 0 else jnp.where(low, swap(g5), v5)
        w[pl.ds(at, 64), 1280:1408] = mixed.astype(BF16)

    def slot(oy, ox):
        return (y + oy + 4) % 4, (x + ox + 4) % 4

    def gv(first, rows, h):
        def ref(oa, ob):
            yy, xx = slot(ob, oa) if first == "x" else slot(oa, ob)
            at = (yy * 4 + xx) * 64 if first == "x" else 1024 + (xx * 4 + yy) * 64
            return w.at[pl.ds(pl.multiple_of(at + h * rows, rows), rows)]

        return ref

    def dn(first, rows, h):
        def ref(oa, ob):
            yy, xx = slot(ob, oa) if first == "x" else slot(oa, ob)
            at = (0 if first == "x" else 352) + h * rows
            return d.at[at:at + rows, pl.ds(pl.multiple_of((yy * 4 + xx) * 128, 128), 128)]

        return ref

    items = []
    for i, (make, rows, first) in enumerate(((gv, 64, "x"), (gv, 64, "y"), (dn, 352, "x"), (dn, 352, "y"))):
        halves = [make(first, rows // 2, h) for h in (0, 1)]
        half = lambda oa, ob, h, halves=halves: halves[h](oa, ob)
        a, b = (to_x, to_y) if first == "x" else (to_y, to_x)
        items.append(ring_copies(make(first, rows, 0), half, a, b, ag_s.at[i], ag_r.at[i]))
    A, B, C, E = items

    def send(item, *which):
        for i in which:
            item[i].start()

    def recv(item, *which):
        for i in which:
            item[i].arrived()

    def rows_of(ref, at, n):
        return ref.at[pl.ds(pl.multiple_of(at, n), n)]

    zw = []
    for h, way in ((0, 1), (1, -1)):
        src = w.at[2048 + 32 * h:2080 + 32 * h]
        dst = rows_of(w, 1024 + (x * 4 + y) * 64 + 32 * h, 32)
        zw.append(Copy(src, dst, dst, zw_s.at[h], zw_r.at[h], to_z[way]))
    for h, way in ((0, 1), (1, -1)):
        part = pl.ds(352 * h, 352)
        zw.append(Copy(dd.at[1 - zlo, part], dz.at[part], dz.at[part], zw_s.at[2 + h], zw_r.at[2 + h], to_z[way]))

    pl.semaphore_wait(barrier, 7)
    send(A, 0, 1)
    zw[0].start()
    zw[1].start()
    send(A, 4, 8)

    loads[2].wait()
    loads[3].wait()
    for i in range(11):
        turned = wd[:, i * 128:(i + 1) * 128].astype(F32).T.astype(BF16)
        at = i * 128
        if i < 5:
            dd[0, at:at + 128] = turned
        elif i == 5:
            dd[0, 640:704] = turned[0:64]
            dd[1, 640:704] = turned[64:128]
        else:
            dd[1, at - 768:at - 640] = turned
    zw[2].start()
    zw[3].start()

    def group_rows(at, n):
        return t.at[:, pl.ds(at, n)]

    tok_z, tok_c, tok_f = [], [], []
    for c in range(4):
        r = 128 * c
        here = group_rows(1024 + r, 128)
        tok_z.append(Copy(group_rows(SENT + r, 128), here, here, tk_s.at[c], tk_r.at[c], to_z[1 if c < 2 else -1]))
        here = group_rows(512 + r, 128)
        tok_c.append(Copy(group_rows(r, 128), here, here, tk_s.at[4 + c], tk_r.at[4 + c], partner))
        here = group_rows(1536 + r, 128)
        tok_f.append(Copy(group_rows(1024 + r, 128), here, here, tk_s.at[8 + c], tk_r.at[8 + c], partner))
    loads[4].wait()
    gain = pre_ref[...].astype(F32)
    low32 = lax.broadcasted_iota(jnp.int32, (32, 128), 1) < 64

    def norm(r):
        v = tok[pl.ds(r, 32), :].astype(F32)
        v = v * lax.rsqrt(jnp.mean(v * v, axis=-1, keepdims=True) + EPS) * gain
        for k in (0, 1):
            straight = pl.multiple_of((zlo + k) % 2 * SENT + r, 32)
            turned = pl.multiple_of((zlo + k + 1) % 2 * SENT + r, 32)
            tiles = [v[:, k * 1024 + 128 * i:k * 1024 + 128 * (i + 1)] for i in range(8)]
            flipped = [swap(s) for s in tiles]
            for i in range(8):
                t[i // 2, pl.ds(straight, 32), 128 * (i % 2):128 * (i % 2 + 1)] = tiles[i].astype(BF16)
            for xx in range(4):
                for p in (0, 1):
                    one, two = 4 * p + xx // 2, 4 * p + 2 + xx // 2
                    if xx % 2 == 0:
                        out = jnp.where(low32, tiles[one], flipped[two])
                    else:
                        out = jnp.where(low32, flipped[one], tiles[two])
                    t[4 + xx, pl.ds(turned, 32), 128 * p:128 * (p + 1)] = out.astype(BF16)

    for c in (0, 2, 1, 3):
        pl.loop(0, 4)(lambda i, c=c: norm(pl.multiple_of(c * 128 + i * 32, 32)))
        tok_z[c].start()
        tok_c[c].start()
        if c == 2:
            zw[0].arrived()
            zw[1].arrived()
            send(B, 0, 1, 4, 8)
            recv(A, 0, 1)
            send(A, 2, 3, 5, 9)

    def gates(groups, row, count, first):
        def step(i):
            r = pl.multiple_of(row + i * 512, 512)
            for n in range(0, F, 256):
                m = min(256, F - n)
                total = None if first else acc[pl.ds(r, 512), n:n + m]
                for g in groups:
                    part = jnp.dot(t[g, pl.ds(r, 512), :], w[pl.ds(pl.multiple_of(g * 256, 256), 256), n:n + m],
                                   preferred_element_type=F32)
                    total = part if total is None else total + part
                acc[pl.ds(r, 512), n:n + m] = total

        pl.loop(0, count // 512)(step)

    recv(B, 0, 1)
    send(B, 2, 3, 5, 9)
    send(A, 6, 10)
    send(B, 6, 10)
    recv(A, 4, 8)
    send(A, 12, 16)
    recv(B, 4, 8)
    send(B, 12, 16)

    zw[2].arrived()
    zw[3].arrived()
    tile0 = pl.multiple_of((y * 4 + x) * 128, 128)
    own_half = (lax.broadcasted_iota(jnp.int32, (Q, 128), 1) < 64) == (zlo == 0)
    d[0:Q, pl.ds(tile0, 128)] = jnp.where(own_half, dd[zlo].astype(F32), dz[...].astype(F32)).astype(BF16)
    d[Q:768, :] = jnp.zeros((64, D), BF16)

    for c in range(4):
        tok_c[c].arrived()
    recv(A, 2, 3)
    send(A, 7, 11)
    recv(B, 2, 3)
    send(B, 7, 11)
    for c in (0, 2):
        tok_z[c].arrived()
        tok_f[c].start()
    gates((y, 4 + x), 0, 1024, True)
    recv(A, 5, 9)
    send(A, 13, 17)
    recv(B, 5, 9)
    send(B, 13, 17)
    recv(A, 6, 10)
    send(A, 14, 18)
    recv(B, 6, 10)
    send(B, 14, 18)
    for c in (1, 3):
        tok_z[c].arrived()
        tok_f[c].start()
    recv(A, 7, 11)
    send(A, 15, 19)
    recv(B, 7, 11)
    send(B, 15, 19)
    send(C, 0, 1)
    send(E, 0, 1)
    send(C, 4, 8)
    send(E, 4, 8)
    for c in range(4):
        tok_f[c].arrived()
    gates((y, 4 + x), 1024, 1024, True)
    up, dn_, rt, lf = (y + 1) % 4, (y + 3) % 4, (x + 1) % 4, (x + 3) % 4
    near = (up, dn_, 4 + rt, 4 + lf)
    gates(near, 1024, 1024, False)
    recv(A, 12, 16, 13, 17, 14, 18, 15, 19)
    recv(B, 12, 16, 13, 17, 14, 18, 15, 19)
    far = ((y + 2) % 4, 4 + (x + 2) % 4)
    gates(far, 1024, 1024, False)

    low128 = lax.broadcasted_iota(jnp.int32, (128, 128), 1) < 64

    def hide(row, count):
        def step(i):
            r = pl.multiple_of(row + i * 128, 128)
            for n in range(0, 640, 128):
                g = acc[pl.ds(r, 128), n:n + 128]
                h = g / (1 + jnp.exp(-g)) * acc[pl.ds(r, 128), 640 + n:768 + n]
                hid[pl.ds(r, 128), n:n + 128] = h.astype(BF16)
            m = acc[pl.ds(r, 128), 1280:1408]
            h = m / (1 + jnp.exp(-m)) * swap(m)
            hid[pl.ds(r, 128), 640:768] = jnp.where(low128, h, 0).astype(BF16)

        pl.loop(0, count // 128)(step)

    hide(1024, 1024)

    def tile_of(oy, ox):
        yy, xx = slot(oy, ox)
        return yy * 4 + xx

    back = []
    tiles = [(0, 0), (0, 1), (0, -1), (1, 0), (-1, 0), (1, 1), (1, -1), (-1, 1), (-1, -1), (0, 2), (2, 0), (2, 1), (2, -1),
             (1, 2), (-1, 2), (2, 2)]

    def remote(k):
        j = tile_of(*tiles[k])
        cols = pl.ds(pl.multiple_of(j * 128, 128), 128)

        def part(row):
            return jnp.dot(hid[row:row + 512, :], d[:, cols], preferred_element_type=F32).astype(BF16)

        ps[j] = part(1536)
        over = Copy(ps.at[j], pr.at[j], pr.at[j], p2_s.at[3 * k], p2_r.at[3 * k], partner)
        over.start()
        rp[j] = part(1024)
        home = [Copy(zs.at[j, h], zr.at[j, h], zr.at[j, h], p2_s.at[3 * k + 1 + h], p2_r.at[3 * k + 1 + h], to_z[way])
                for h, way in ((0, -1), (1, 1))]
        back.append((j, over, home))

    def pass_on(k):
        j, over, home = back[k]
        over.arrived()
        both = (rp[j].astype(F32) + pr[j].astype(F32)).astype(BF16)
        zs[j, 0] = both[0:256]
        zs[j, 1] = both[256:512]
        home[0].start()
        home[1].start()

    def run(ks):
        for k in ks:
            remote(k)
            if k > 0:
                pass_on(k - 1)

    run([0])
    recv(C, 0, 1)
    send(C, 2, 3, 5, 9)
    recv(E, 0, 1)
    send(E, 2, 3, 5, 9)
    send(C, 6, 10)
    send(E, 6, 10)
    recv(C, 4, 8)
    send(C, 12, 16)
    recv(E, 4, 8)
    send(E, 12, 16)
    run([1, 2, 3, 4])
    recv(C, 2, 3)
    send(C, 7, 11)
    recv(E, 2, 3)
    send(E, 7, 11)
    recv(C, 5, 9)
    send(C, 13, 17)
    recv(E, 5, 9)
    send(E, 13, 17)
    recv(C, 6, 10)
    send(C, 14, 18)
    recv(E, 6, 10)
    send(E, 14, 18)
    run([5, 6, 7, 8])
    recv(C, 7, 11)
    send(C, 15, 19)
    recv(E, 7, 11)
    send(E, 15, 19)
    recv(C, 12, 16)
    recv(E, 12, 16)
    run([9, 10])
    recv(C, 13, 14, 15, 17, 18, 19)
    recv(E, 13, 14, 15, 17, 18, 19)
    run([11, 12, 13, 14, 15])
    pass_on(15)

    gates(near + far, 0, 1024, False)
    hide(0, 1024)
    across = []
    for n in range(8):
        cols = slice(256 * n, 256 * (n + 1))
        os_[:, cols] = jnp.dot(hid[512:1024, :], d[:, cols], preferred_element_type=F32).astype(BF16)
        across.append(Copy(os_.at[:, cols], or_.at[:, cols], or_.at[:, cols], p2_s.at[48 + n], p2_r.at[48 + n], partner))
        across[n].start()
        own[:, cols] = jnp.dot(hid[0:512, :], d[:, cols], preferred_element_type=F32).astype(BF16)
    for c in across:
        c.arrived()
    for _, _, home in back:
        home[0].arrived()
        home[1].arrived()

    post = post_ref[...].astype(F32)
    low16 = lax.broadcasted_iota(jnp.int32, (16, 128), 1) < 64

    def finish(h, i):
        r = pl.multiple_of(i * 16, 16)
        row = pl.multiple_of(h * 256 + r, 16)
        b, square = [], jnp.zeros((16, 128), F32)
        for j in range(16):
            cols = slice(128 * j, 128 * (j + 1))
            v = own[pl.ds(row, 16), cols].astype(F32) + or_[pl.ds(row, 16), cols].astype(F32)
            v = (v + zr[j, h, pl.ds(r, 16), :].astype(F32)).astype(BF16).astype(F32)
            square += v * v
            b.append(v)
        scale = 0.5 * lax.rsqrt(jnp.sum(square, axis=-1, keepdims=True) * (1 / D) + EPS)
        for j in range(16):
            one, two = b[2 * (j % 8)], b[2 * (j % 8) + 1]
            v = jnp.where(low16, one, swap(two)) if j < 8 else jnp.where(low16, swap(one), two)
            cols = slice(128 * j, 128 * (j + 1))
            v = tok[pl.ds(row, 16), cols].astype(F32) + v * scale * post[:, cols]
            tok[pl.ds(row, 16), cols] = v.astype(BF16)

    stores = []
    for h in (0, 1):
        pl.loop(0, 16)(lambda i, h=h: finish(h, i))
        rows = pl.ds(256 * h, 256)
        stores.append(pltpu.make_async_copy(tok.at[rows], out_ref.at[rows], load.at[5 + h]))
        stores[h].start()

    for c in A + B + C + E + zw + tok_z + tok_c + tok_f + across:
        c.left()
    for _, over, home in back:
        over.left()
        home[0].left()
        home[1].left()
    for c in stores:
        c.wait()


def shards(tokens, pre_gain, gate_weight, value_weight, down_weight, post_gain):
    any_, vmem = pl.BlockSpec(memory_space=pl.ANY), pl.BlockSpec(memory_space=pltpu.VMEM)
    sem = pltpu.SemaphoreType.DMA
    buf = lambda *s, t=BF16: pltpu.VMEM(s, t)
    return pl.pallas_call(
        kernel,
        out_shape=jax.ShapeDtypeStruct((TOK, D), BF16),
        in_specs=[any_, vmem, any_, any_, any_, vmem],
        out_specs=any_,
        scratch_shapes=[
            buf(TOK, D), buf(64, F), buf(64, F), buf(128, F), buf(2, Q, 128), buf(Q, 128), buf(2112, F), buf(768, D),
            buf(8, 2560, 256), buf(2048, F, t=F32), buf(2048, 768), buf(16, 512, 128), buf(16, 512, 128), buf(16, 512, 128),
            buf(16, 2, 256, 128), buf(16, 2, 256, 128), buf(TOK, D), buf(TOK, D), buf(TOK, D),
            sem((7,)), sem((4, 20)), sem((4, 20)), sem((4,)), sem((4,)), sem((12,)), sem((12,)), sem((56,)), sem((56,)),
        ],
        compiler_params=pltpu.CompilerParams(collective_id=0, has_side_effects=True, vmem_limit_bytes=63 * 1024 * 1024),
    )(tokens, pre_gain[None], gate_weight, value_weight, down_weight.T, post_gain[None])


def solution(mesh):
    rows = P(("rep", "fs", "tp"), None)
    in_specs = (rows, P(), P("fs", "tp"), P("fs", "tp"), P("tp", "fs"), P())
    return jax.shard_map(shards, mesh=mesh, in_specs=in_specs, out_specs=rows, check_vma=False)
```

```python
import jax
import jax.numpy as jnp
from jax import lax
from jax.experimental import pallas as pl
from jax.experimental.pallas import tpu as pltpu
from jax.sharding import PartitionSpec as P

D, F, Q, TOK = 2048, 1408, 704, 512
SENT = 2048
EPS = 1e-06
F32, BF16 = jnp.float32, jnp.bfloat16


class Copy:
    def __init__(self, src, dst, here, send_sem, recv_sem, to):
        make = pltpu.make_async_remote_copy
        kind = dict(device_id=to, device_id_type=pl.DeviceIdType.MESH)
        self.out = make(src_ref=src, dst_ref=dst, send_sem=send_sem, recv_sem=recv_sem, **kind)
        self.into = make(src_ref=here, dst_ref=here, send_sem=send_sem, recv_sem=recv_sem, **kind)

    def start(self):
        self.out.start()

    def arrived(self):
        self.into.wait_recv()

    def left(self):
        self.out.wait_send()


def ring_copies(block, half, to_a, to_b, send, recv):
    c = []
    for way in (1, -1):
        c.append((block(0, 0, 0, 0), block(0, 0, way, 0), block(-way, 0, 0, 0), to_a[way]))
    for way, h in ((1, 0), (-1, 1)):
        c.append((half(-way, 0, 0, 0, h), half(-way, 0, way, 0, h), half(2, 0, 0, 0, h), to_a[way]))
    for way in (1, -1):
        for oa in (0, -1, 1, 2):
            c.append((block(oa, 0, 0, 0), block(oa, 0, 0, way), block(oa, -way, 0, 0), to_b[way]))
    for way, h in ((1, 0), (-1, 1)):
        for oa in (0, -1, 1, 2):
            c.append((half(oa, -way, 0, 0, h), half(oa, -way, 0, way, h), half(oa, 2, 0, 0, h), to_b[way]))
    return [Copy(src, dst, here, send.at[i], recv.at[i], to) for i, (src, dst, here, to) in enumerate(c)]


def position(offset):
    return (0, 1, 3, 2)[offset % 4]


def kernel(tok_in, pre_ref, gate_in, value_in, down_in, post_ref, out_ref, tok, wg, wv, wd, dd, dz, w, d, t, acc, hid, ps,
           pr, rp, zs, zr, own, os_, or_, load, ag_s, ag_r, zw_s, zw_r, tk_s, tk_r, p2_s, p2_r):
    rep, fs, core = lax.axis_index("rep"), lax.axis_index("fs"), lax.axis_index("tp")
    zlo, y, x = fs // 16, (fs // 4) % 4, fs % 4
    z = rep * 2 + zlo

    def device(dz_=0, dy=0, dx=0, other=False):
        zz, yy, xx = (z + dz_ + 4) % 4, (y + dy + 4) % 4, (x + dx + 4) % 4
        return {"rep": zz // 2, "fs": (zz % 2) * 16 + yy * 4 + xx, "tp": 1 - core if other else core}

    to_x = {1: device(dx=1), -1: device(dx=-1)}
    to_y = {1: device(dy=1), -1: device(dy=-1)}
    to_z = {1: device(dz_=1), -1: device(dz_=-1)}
    partner = device(other=True)

    loads = [
        pltpu.make_async_copy(gate_in, wg, load.at[0]),
        pltpu.make_async_copy(value_in, wv, load.at[1]),
        pltpu.make_async_copy(down_in, wd.at[0:64], load.at[2]),
        pltpu.make_async_copy(down_in, wd.at[64:128], load.at[3]),
    ] + [pltpu.make_async_copy(tok_in.at[128 * c:128 * c + 128], tok.at[128 * c:128 * c + 128], load.at[4 + c]) for c in range(4)]
    for c in loads:
        c.start()

    barrier = pltpu.get_barrier_semaphore()
    for peer in (*to_x.values(), *to_y.values(), *to_z.values(), partner):
        pl.semaphore_signal(barrier, inc=1, device_id=peer, device_id_type=pl.DeviceIdType.MESH)

    lanes = lax.broadcasted_iota(jnp.int32, (64, 128), 1)
    low = lanes < 64
    swap = lambda v: pltpu.roll(v, 64, 1)

    loads[0].wait()
    loads[1].wait()
    place = (y * 4 + x) * 64
    for q in (0, 1):
        at = pl.multiple_of(place + (zlo + q) % 2 * (2048 - place), 64)
        g5, v5 = wg[:, 640:768].astype(F32), wv[:, 640:768].astype(F32)
        first = 768 * q
        w[pl.ds(at, 64), 0:640] = wg[:, first:first + 640]
        w[pl.ds(at, 64), 640:1280] = wv[:, first:first + 640]
        mixed = jnp.where(low, g5, swap(v5)) if q == 0 else jnp.where(low, swap(g5), v5)
        w[pl.ds(at, 64), 1280:1408] = mixed.astype(BF16)

    def slot(oy, ox):
        return (y + oy + 4) % 4, (x + ox + 4) % 4

    def gv(first, rows, h):
        def ref(oa, ob, ma, mb):
            yy, xx = slot(ob, oa) if first == "x" else slot(oa, ob)
            at = (yy * 4 + xx) * 64 if first == "x" else 1024 + (xx * 4 + yy) * 64
            return w.at[pl.ds(pl.multiple_of(at + h * rows, rows), rows)]

        return ref

    def dn(first, rows, h):
        def ref(oa, ob, ma, mb):
            oa, ob = position(oa - ma), position(ob - mb)
            at = (0 if first == "x" else 352) + h * rows
            n = (ob * 4 + oa if first == "x" else oa * 4 + ob) * 128
            return d.at[at:at + rows, n:n + 128]

        return ref

    items = []
    for i, (make, rows, first) in enumerate(((gv, 64, "x"), (gv, 64, "y"), (dn, 352, "x"), (dn, 352, "y"))):
        halves = [make(first, rows // 2, h) for h in (0, 1)]
        half = lambda oa, ob, ma, mb, h, halves=halves: halves[h](oa, ob, ma, mb)
        a, b = (to_x, to_y) if first == "x" else (to_y, to_x)
        items.append(ring_copies(make(first, rows, 0), half, a, b, ag_s.at[i], ag_r.at[i]))
    A, B, C, E = items

    def send(item, *which):
        for i in which:
            item[i].start()

    def recv(item, *which):
        for i in which:
            item[i].arrived()

    def rows_of(ref, at, n):
        return ref.at[pl.ds(pl.multiple_of(at, n), n)]

    zw = []
    for h, way in ((0, 1), (1, -1)):
        src = w.at[2048 + 32 * h:2080 + 32 * h]
        dst = rows_of(w, 1024 + (x * 4 + y) * 64 + 32 * h, 32)
        zw.append(Copy(src, dst, dst, zw_s.at[h], zw_r.at[h], to_z[way]))
    for h, way in ((0, 1), (1, -1)):
        part = pl.ds(352 * h, 352)
        zw.append(Copy(dd.at[1 - zlo, part], dz.at[part], dz.at[part], zw_s.at[2 + h], zw_r.at[2 + h], to_z[way]))

    def group_rows(at):
        return t.at[:, pl.ds(at, 128)]

    tok_z, tok_c, tok_f = [], [], []
    for c in range(4):
        r = 128 * c
        mine = 1024 + 512 * (c % 2) + 128 * (c // 2)
        here = group_rows(mine)
        tok_z.append(Copy(group_rows(SENT + r), here, here, tk_s.at[c], tk_r.at[c], to_z[1 if c < 2 else -1]))
        here = group_rows(512 + r)
        tok_c.append(Copy(group_rows(r), here, here, tk_s.at[4 + c], tk_r.at[4 + c], partner))
        here = group_rows(mine + 256)
        tok_f.append(Copy(group_rows(mine), here, here, tk_s.at[8 + c], tk_r.at[8 + c], partner))
    gain = pre_ref[...].astype(F32).reshape(1, D)
    low32 = lax.broadcasted_iota(jnp.int32, (32, 128), 1) < 64

    def norm_rows(r):
        v = tok[pl.ds(r, 32), :].astype(F32)
        v = v * lax.rsqrt(jnp.mean(v * v, axis=-1, keepdims=True) + EPS) * gain
        for k in (0, 1):
            straight = pl.multiple_of((zlo + k) % 2 * SENT + r, 32)
            turned = pl.multiple_of((zlo + k + 1) % 2 * SENT + r, 32)
            tiles = [v[:, k * 1024 + 128 * i:k * 1024 + 128 * (i + 1)] for i in range(8)]
            flipped = [swap(s) for s in tiles]
            for i in range(8):
                t[i // 2, pl.ds(straight, 32), 128 * (i % 2):128 * (i % 2 + 1)] = tiles[i].astype(BF16)
            for xx in range(4):
                for p in (0, 1):
                    one, two = 4 * p + xx // 2, 4 * p + 2 + xx // 2
                    if xx % 2 == 0:
                        out = jnp.where(low32, tiles[one], flipped[two])
                    else:
                        out = jnp.where(low32, flipped[one], tiles[two])
                    t[4 + xx, pl.ds(turned, 32), 128 * p:128 * (p + 1)] = out.astype(BF16)

    def norm(c):
        loads[4 + c].wait()
        pl.loop(0, 4)(lambda i: norm_rows(pl.multiple_of(c * 128 + i * 32, 32)))

    def gates(groups, row, count, first):
        def step(i):
            r = pl.multiple_of(row + i * 512, 512)
            for n in range(0, F, 256):
                m = min(256, F - n)
                total = None if first else acc[pl.ds(r, 512), n:n + m]
                for g in groups:
                    part = jnp.dot(t[g, pl.ds(r, 512), :], w[pl.ds(pl.multiple_of(g * 256, 256), 256), n:n + m],
                                   preferred_element_type=F32)
                    total = part if total is None else total + part
                acc[pl.ds(r, 512), n:n + m] = total

        pl.loop(0, count // 512)(step)

    low128 = lax.broadcasted_iota(jnp.int32, (128, 128), 1) < 64

    def hide(row, count):
        def step(i):
            r = pl.multiple_of(row + i * 128, 128)
            for n in range(0, 640, 128):
                g = acc[pl.ds(r, 128), n:n + 128]
                h = g / (1 + jnp.exp(-g)) * acc[pl.ds(r, 128), 640 + n:768 + n]
                hid[pl.ds(r, 128), n:n + 128] = h.astype(BF16)
            m = acc[pl.ds(r, 128), 1280:1408]
            h = m / (1 + jnp.exp(-m)) * swap(m)
            hid[pl.ds(r, 128), 640:768] = jnp.where(low128, h, 0).astype(BF16)

        pl.loop(0, count // 128)(step)

    pending, back = [], []

    def remote(s, rows, cols):
        ys, xs = range(4)[rows], range(4)[cols]
        slots = [(py, px) for py in ys for px in xs]
        for i in range(0, len(slots), 2):
            pair = slots[i:i + 2]
            right = [d[:, (py * 4 + px) * 128:(py * 4 + px + 1) * 128] for py, px in pair]
            right = jnp.concatenate(right, axis=1) if len(pair) == 2 else right[0]
            part = jnp.dot(hid[1024 + 512 * s:1536 + 512 * s, :], right, preferred_element_type=F32).astype(BF16)
            for n, (py, px) in enumerate(pair):
                ps[s, py, px] = part[256:512, 128 * n:128 * (n + 1)]
                rp[s, py, px] = part[0:256, 128 * n:128 * (n + 1)]
        k = 3 * len(back)
        here = pr.at[s, rows, cols]
        over = Copy(ps.at[s, rows, cols], here, here, p2_s.at[k], p2_r.at[k], partner)
        over.start()
        home = []
        for h, way in ((0, -1), (1, 1)):
            here = zr.at[s, h, rows, cols]
            home.append(Copy(zs.at[s, h, rows, cols], here, here, p2_s.at[k + 1 + h], p2_r.at[k + 1 + h], to_z[way]))
        back.append((s, over, home))
        pending.append((s, slots, over, home))
        if len(pending) > 1:
            pass_on()

    def pass_on():
        s, slots, over, home = pending.pop(0)
        over.arrived()
        for py, px in slots:
            both = (rp[s, py, px].astype(F32) + pr[s, py, px].astype(F32)).astype(BF16)
            zs[s, 0, py, px] = both[0:128]
            zs[s, 1, py, px] = both[128:256]
        home[0].start()
        home[1].start()

    norm(0)
    pl.semaphore_wait(barrier, 7)
    zw[0].start()
    zw[1].start()
    send(A, 0, 1, 4, 8)
    tok_z[0].start()
    tok_c[0].start()
    for c in (2, 1, 3):
        norm(c)
        tok_z[c].start()
        tok_c[c].start()

    loads[2].wait()
    loads[3].wait()
    for i in range(11):
        turned = wd[:, i * 128:(i + 1) * 128].astype(F32).T.astype(BF16)
        at = i * 128
        if i < 5:
            dd[0, at:at + 128] = turned
        elif i == 5:
            dd[0, 640:704] = turned[0:64]
            dd[1, 640:704] = turned[64:128]
        else:
            dd[1, at - 768:at - 640] = turned
    zw[2].start()
    zw[3].start()
    d[Q:768, :] = jnp.zeros((64, D), BF16)

    zw[0].arrived()
    zw[1].arrived()
    send(B, 0, 1, 4, 8)
    recv(A, 0, 1)
    send(A, 2, 3, 5, 9)
    recv(B, 0, 1)
    send(B, 2, 3, 5, 9)
    recv(A, 4, 8)
    send(A, 6, 10, 12, 16)
    recv(B, 4, 8)
    send(B, 6, 10, 12, 16)
    for c in range(4):
        tok_c[c].arrived()
    recv(A, 2, 3)
    send(A, 7, 11)
    recv(A, 5, 9)
    send(A, 13, 17)
    recv(B, 2, 3)
    send(B, 7, 11)
    recv(B, 5, 9)
    send(B, 13, 17)
    here, near, far = (y, 4 + x), ((y + 1) % 4, (y + 3) % 4, 4 + (x + 1) % 4, 4 + (x + 3) % 4), ((y + 2) % 4, 4 + (x + 2) % 4)
    gates(here, 0, 512, True)
    tok_z[0].arrived()
    tok_f[0].start()
    tok_z[2].arrived()
    tok_f[2].start()
    recv(A, 6, 10)
    send(A, 14, 18)
    recv(B, 6, 10)
    send(B, 14, 18)
    gates(here, 512, 512, True)
    tok_f[0].arrived()
    tok_f[2].arrived()
    gates(here, 1024, 512, True)
    recv(A, 7, 11)
    send(A, 15, 19)
    recv(B, 7, 11)
    send(B, 15, 19)
    gates(near, 1024, 512, False)
    tok_z[1].arrived()
    tok_f[1].start()
    tok_z[3].arrived()
    tok_f[3].start()

    zw[2].arrived()
    zw[3].arrived()
    own_half = (lax.broadcasted_iota(jnp.int32, (Q, 128), 1) < 64) == (zlo == 0)
    d[0:Q, 0:128] = jnp.where(own_half, dd[zlo].astype(F32), dz[...].astype(F32)).astype(BF16)
    send(C, 0, 1)
    send(E, 0, 1)
    send(C, 4, 8)
    send(E, 4, 8)
    tok_f[1].arrived()
    tok_f[3].arrived()
    gates(here + near, 1536, 512, True)
    recv(A, 12, 16, 13, 17, 14, 18, 15, 19)
    recv(B, 12, 16, 13, 17, 14, 18, 15, 19)
    one, two, last = slice(0, 1), slice(1, 3), slice(3, 4)
    gates(far, 1024, 512, False)
    hide(1024, 512)
    remote(0, one, one)
    gates(far, 1536, 512, False)
    hide(1536, 512)
    remote(1, one, one)
    recv(C, 0, 1)
    send(C, 2, 3, 5, 9)
    recv(E, 0, 1)
    send(E, 2, 3, 5, 9)
    recv(C, 4, 8)
    send(C, 6, 10, 12, 16)
    recv(E, 4, 8)
    send(E, 6, 10, 12, 16)
    for s in (0, 1):
        remote(s, one, two)
        remote(s, two, one)
    recv(C, 2, 3)
    send(C, 7, 11)
    recv(E, 2, 3)
    send(E, 7, 11)
    recv(C, 5, 9)
    send(C, 13, 17)
    recv(E, 5, 9)
    send(E, 13, 17)
    pass_on()
    gates(near, 0, 512, False)
    recv(C, 6, 10)
    send(C, 14, 18)
    recv(E, 6, 10)
    send(E, 14, 18)
    for s in (0, 1):
        remote(s, two, two)
    pass_on()
    recv(C, 7, 11)
    send(C, 15, 19)
    recv(E, 7, 11)
    send(E, 15, 19)
    gates(near, 512, 512, False)
    recv(C, 12, 16)
    recv(E, 12, 16)
    remote(0, one, last)
    remote(0, last, one)
    pass_on()
    gates(far, 0, 1024, False)
    recv(C, 13, 14, 15, 17, 18, 19)
    recv(E, 13, 14, 15, 17, 18, 19)
    remote(0, two, last)
    remote(0, last, two)
    remote(0, last, last)
    remote(1, one, last)
    remote(1, last, one)
    remote(1, two, last)
    remote(1, last, two)
    remote(1, last, last)
    pass_on()

    hide(0, 1024)
    across = []
    for n in range(8):
        cols = slice(256 * n, 256 * (n + 1))
        os_[:, cols] = jnp.dot(hid[512:1024, :], d[:, cols], preferred_element_type=F32).astype(BF16)
        across.append(Copy(os_.at[:, cols], or_.at[:, cols], or_.at[:, cols], p2_s.at[54 + n], p2_r.at[54 + n], partner))
        across[n].start()
        own[:, cols] = jnp.dot(hid[0:512, :], d[:, cols], preferred_element_type=F32).astype(BF16)
    for c in across:
        c.arrived()

    post = post_ref[...].astype(F32).reshape(1, D)
    low16 = lax.broadcasted_iota(jnp.int32, (16, 128), 1) < 64

    def spot(theirs, me):
        o = (theirs - me + 4) % 4
        return o + o // 2 - o // 3 * 2

    spots = [(spot(j // 4, y), spot(j % 4, x)) for j in range(16)]

    def finish(s, h, i):
        r = pl.multiple_of(i * 16, 16)
        row = pl.multiple_of((2 * h + s) * 128 + r, 16)
        b, square = [], jnp.zeros((16, 128), F32)
        for py, px in spots:
            cols = pl.ds(pl.multiple_of((py * 4 + px) * 128, 128), 128)
            v = own[pl.ds(row, 16), cols].astype(F32) + or_[pl.ds(row, 16), cols].astype(F32)
            v = (v + zr[s, h, py, px, pl.ds(r, 16), :].astype(F32)).astype(BF16).astype(F32)
            square += v * v
            b.append(v)
        scale = 0.5 * lax.rsqrt(jnp.sum(square, axis=-1, keepdims=True) * (1 / D) + EPS)
        for j in range(16):
            one, two = b[2 * (j % 8)], b[2 * (j % 8) + 1]
            v = jnp.where(low16, one, swap(two)) if j < 8 else jnp.where(low16, swap(one), two)
            cols = slice(128 * j, 128 * (j + 1))
            v = tok[pl.ds(row, 16), cols].astype(F32) + v * scale * post[:, cols]
            tok[pl.ds(row, 16), cols] = v.astype(BF16)

    stores = []
    for half in (0, 1):
        for s, _, home in back:
            if s == half:
                home[0].arrived()
                home[1].arrived()
        for h in (0, 1):
            pl.loop(0, 8)(lambda i, h=h, half=half: finish(half, h, i))
            rows = pl.ds((2 * h + half) * 128, 128)
            stores.append(pltpu.make_async_copy(tok.at[rows], out_ref.at[rows], load.at[8 + len(stores)]))
            stores[-1].start()

    for c in A + B + C + E + zw + tok_z + tok_c + tok_f + across:
        c.left()
    for _, over, home in back:
        over.left()
        home[0].left()
        home[1].left()
    for c in stores:
        c.wait()


def shards(tokens, pre_gain, gate_weight, value_weight, down_weight, post_gain):
    any_, vmem = pl.BlockSpec(memory_space=pl.ANY), pl.BlockSpec(memory_space=pltpu.VMEM)
    sem = pltpu.SemaphoreType.DMA
    buf = lambda *s, t=BF16: pltpu.VMEM(s, t)
    return pl.pallas_call(
        kernel,
        out_shape=jax.ShapeDtypeStruct((TOK, D), BF16),
        in_specs=[any_, vmem, any_, any_, any_, vmem],
        out_specs=any_,
        scratch_shapes=[
            buf(TOK, D), buf(64, F), buf(64, F), buf(128, F), buf(2, Q, 128), buf(Q, 128), buf(2112, F), buf(768, D),
            buf(8, 2560, 256), buf(2048, F, t=F32), buf(2048, 768), *[buf(2, 4, 4, 256, 128)] * 3, *[buf(2, 2, 4, 4, 128, 128)] * 2,
            buf(TOK, D), buf(TOK, D), buf(TOK, D),
            sem((12,)), sem((4, 20)), sem((4, 20)), sem((4,)), sem((4,)), sem((12,)), sem((12,)), sem((62,)), sem((62,)),
        ],
        compiler_params=pltpu.CompilerParams(collective_id=0, has_side_effects=True, vmem_limit_bytes=63 * 1024 * 1024),
    )(tokens, pre_gain, gate_weight, value_weight, down_weight.T, post_gain)


def solution(mesh):
    rows = P(("rep", "fs", "tp"), None)
    in_specs = (rows, P(), P("fs", "tp"), P("fs", "tp"), P("tp", "fs"), P())
    return jax.shard_map(shards, mesh=mesh, in_specs=in_specs, out_specs=rows, check_vma=False)
```

```python
import jax
import jax.numpy as jnp
from jax import lax
from jax.experimental import pallas as pl
from jax.experimental.pallas import tpu as pltpu
from jax.sharding import PartitionSpec as P

D, F, Q, TOK = 2048, 1408, 704, 512
SENT = 2048
EPS = 1e-06
F32, BF16 = jnp.float32, jnp.bfloat16


def remote_copy(src, dst, send_sem, recv_sem, to):
    return pltpu.make_async_remote_copy(src_ref=src, dst_ref=dst, send_sem=send_sem, recv_sem=recv_sem, device_id=to,
                                        device_id_type=pl.DeviceIdType.MESH)


TOGETHER = {0: (0, 2), 1: (0, 2), 4: (1, 2), 8: (1, 2), 2: (2, 1), 3: (2, 1), 5: (3, 2), 9: (3, 2), 6: (4, 2), 10: (4, 2),
            7: (5, 2), 11: (5, 2)}


def ring_copies(block, half, to_a, to_b, send, recv):
    c = []
    for way in (1, -1):
        c.append((block(0, 0, 0, 0), block(0, 0, way, 0), to_a[way]))
    for way, h in ((1, 0), (-1, 1)):
        c.append((half(-way, 0, 0, 0, h), half(-way, 0, way, 0, h), to_a[way]))
    for way in (1, -1):
        for oa in (0, -1, 1, 2):
            c.append((block(oa, 0, 0, 0), block(oa, 0, 0, way), to_b[way]))
    for way, h in ((1, 0), (-1, 1)):
        for oa in (0, -1, 1, 2):
            c.append((half(oa, -way, 0, 0, h), half(oa, -way, 0, way, h), to_b[way]))
    return [remote_copy(src, dst, send, recv(i), to) for i, (src, dst, to) in enumerate(c)]


def position(offset):
    return (0, 1, 3, 2)[offset % 4]


def kernel(tok_in, pre_ref, gate_in, value_in, down_in, post_ref, out_ref, tok, wg, wv, wd, dd, dz, w, d, t, acc, hid, ps,
           pr, rp, zs, zr, os_, or_, load, ag_r, zw_r, tk_r, pr_r, zr_r, or_r, sent):
    rep, fs, core = lax.axis_index("rep"), lax.axis_index("fs"), lax.axis_index("tp")
    zlo, y, x = fs // 16, (fs // 4) % 4, fs % 4
    z = rep * 2 + zlo

    def device(dz_=0, dy=0, dx=0, other=False):
        zz, yy, xx = (z + dz_ + 4) % 4, (y + dy + 4) % 4, (x + dx + 4) % 4
        return {"rep": zz // 2, "fs": (zz % 2) * 16 + yy * 4 + xx, "tp": 1 - core if other else core}

    to_x = {1: device(dx=1), -1: device(dx=-1)}
    to_y = {1: device(dy=1), -1: device(dy=-1)}
    to_z = {1: device(dz_=1), -1: device(dz_=-1)}
    partner = device(other=True)

    loads = [
        pltpu.make_async_copy(gate_in, wg, load.at[0]),
        pltpu.make_async_copy(value_in, wv, load.at[1]),
        pltpu.make_async_copy(down_in, wd.at[0:64], load.at[2]),
        pltpu.make_async_copy(down_in, wd.at[64:128], load.at[3]),
    ] + [pltpu.make_async_copy(tok_in.at[128 * c:128 * c + 128], tok.at[128 * c:128 * c + 128], load.at[4 + c]) for c in range(4)]
    for c in loads:
        c.start()

    barrier = pltpu.get_barrier_semaphore()
    for peer in (*to_x.values(), *to_y.values(), *to_z.values(), partner):
        pl.semaphore_signal(barrier, inc=1, device_id=peer, device_id_type=pl.DeviceIdType.MESH)

    lanes = lax.broadcasted_iota(jnp.int32, (64, 128), 1)
    low = lanes < 64
    swap = lambda v: pltpu.roll(v, 64, 1)

    loads[0].wait()
    loads[1].wait()
    place = (y * 4 + x) * 64
    for q in (0, 1):
        at = pl.multiple_of(place + (zlo + q) % 2 * (2048 - place), 64)
        g5, v5 = wg[:, 640:768].astype(F32), wv[:, 640:768].astype(F32)
        first = 768 * q
        w[pl.ds(at, 64), 0:640] = wg[:, first:first + 640]
        w[pl.ds(at, 64), 640:1280] = wv[:, first:first + 640]
        mixed = jnp.where(low, g5, swap(v5)) if q == 0 else jnp.where(low, swap(g5), v5)
        w[pl.ds(at, 64), 1280:1408] = mixed.astype(BF16)

    def slot(oy, ox):
        return (y + oy + 4) % 4, (x + ox + 4) % 4

    def gv(first, rows, h):
        def ref(oa, ob, ma, mb):
            yy, xx = slot(ob, oa) if first == "x" else slot(oa, ob)
            at = (yy * 4 + xx) * 64 if first == "x" else 1024 + (xx * 4 + yy) * 64
            return w.at[pl.ds(pl.multiple_of(at + h * rows, rows), rows)]

        return ref

    def dn(first, rows, h):
        def ref(oa, ob, ma, mb):
            oa, ob = position(oa - ma), position(ob - mb)
            at = (0 if first == "x" else 352) + h * rows
            n = (ob * 4 + oa if first == "x" else oa * 4 + ob) * 128
            return d.at[at:at + rows, n:n + 128]

        return ref

    def arrived(ref, sem):
        remote_copy(ref, ref, sem, sem, partner).wait_recv()

    def left(ref, sem):
        remote_copy(ref, ref, sem, sem, partner).wait_send()

    def together(i, kind):
        if i in TOGETHER:
            return TOGETHER[i]
        if kind is gv:
            return 6, 4
        return (6, 1) if i in (12, 16) else (7, 3)

    items = []
    for i, (make, rows, first) in enumerate(((gv, 64, "x"), (gv, 64, "y"), (dn, 352, "x"), (dn, 352, "y"))):
        halves = [make(first, rows // 2, h) for h in (0, 1)]
        half = lambda oa, ob, ma, mb, h, halves=halves: halves[h](oa, ob, ma, mb)
        a, b = (to_x, to_y) if first == "x" else (to_y, to_x)
        sem = lambda n, i=i, make=make: ag_r.at[i, together(n, make)[0]]
        items.append((ring_copies(make(first, rows, 0), half, a, b, sent.at[i // 2], sem), make, i))
    A, B, C, E = items

    def send(item, *which):
        for i in which:
            item[0][i].start()

    def recv(item, which):
        group, blocks = together(which, item[1])
        ref = w.at[0:64 * blocks] if item[1] is gv else d.at[0:352, 0:128 * blocks]
        arrived(ref, ag_r.at[item[2], group])

    def rows_of(ref, at, n):
        return ref.at[pl.ds(pl.multiple_of(at, n), n)]

    zw = []
    for h, way in ((0, 1), (1, -1)):
        dst = rows_of(w, 1024 + (x * 4 + y) * 64 + 32 * h, 32)
        zw.append(remote_copy(w.at[2048 + 32 * h:2080 + 32 * h], dst, sent.at[2], zw_r.at[0], to_z[way]))
    for h, way in ((0, 1), (1, -1)):
        part = pl.ds(352 * h, 352)
        zw.append(remote_copy(dd.at[1 - zlo, part], dz.at[part], sent.at[2], zw_r.at[1], to_z[way]))

    def group_rows(at):
        return t.at[:, pl.ds(at, 128)]

    tok_z, tok_c, tok_f = [], [], []
    for c in range(4):
        r = 128 * c
        mine = 1024 + 512 * (c % 2) + 128 * (c // 2)
        tok_z.append(remote_copy(group_rows(SENT + r), group_rows(mine), sent.at[3], tk_r.at[c % 2], to_z[1 if c < 2 else -1]))
        tok_c.append(remote_copy(group_rows(r), group_rows(512 + r), sent.at[3], tk_r.at[2], partner))
        tok_f.append(remote_copy(group_rows(mine), group_rows(mine + 256), sent.at[3], tk_r.at[3 + c % 2], partner))

    def forward(half):
        arrived(t.at[:, 0:256], tk_r.at[half])
        tok_f[half].start()
        tok_f[half + 2].start()

    def forwarded(half):
        arrived(t.at[:, 0:256], tk_r.at[3 + half])

    gain = pre_ref[...].astype(F32).reshape(1, D)
    low32 = lax.broadcasted_iota(jnp.int32, (32, 128), 1) < 64

    def norm_rows(r):
        v = tok[pl.ds(r, 32), :].astype(F32)
        v = v * lax.rsqrt(jnp.mean(v * v, axis=-1, keepdims=True) + EPS) * gain
        for k in (0, 1):
            straight = pl.multiple_of((zlo + k) % 2 * SENT + r, 32)
            turned = pl.multiple_of((zlo + k + 1) % 2 * SENT + r, 32)
            tiles = [v[:, k * 1024 + 128 * i:k * 1024 + 128 * (i + 1)] for i in range(8)]
            flipped = [swap(s) for s in tiles]
            for i in range(8):
                t[i // 2, pl.ds(straight, 32), 128 * (i % 2):128 * (i % 2 + 1)] = tiles[i].astype(BF16)
            for xx in range(4):
                for p in (0, 1):
                    one, two = 4 * p + xx // 2, 4 * p + 2 + xx // 2
                    if xx % 2 == 0:
                        out = jnp.where(low32, tiles[one], flipped[two])
                    else:
                        out = jnp.where(low32, flipped[one], tiles[two])
                    t[4 + xx, pl.ds(turned, 32), 128 * p:128 * (p + 1)] = out.astype(BF16)

    def norm(c):
        loads[4 + c].wait()
        pl.loop(0, 4)(lambda i: norm_rows(pl.multiple_of(c * 128 + i * 32, 32)))

    def gates(groups, row, count, first):
        def step(i):
            r = pl.multiple_of(row + i * 512, 512)
            for n in range(0, F, 256):
                m = min(256, F - n)
                total = None if first else acc[pl.ds(r, 512), n:n + m]
                for g in groups:
                    part = jnp.dot(t[g, pl.ds(r, 512), :], w[pl.ds(pl.multiple_of(g * 256, 256), 256), n:n + m],
                                   preferred_element_type=F32)
                    total = part if total is None else total + part
                acc[pl.ds(r, 512), n:n + m] = total

        pl.loop(0, count // 512)(step)

    low128 = lax.broadcasted_iota(jnp.int32, (128, 128), 1) < 64

    def hide(row, count):
        def step(i):
            r = pl.multiple_of(row + i * 128, 128)
            for n in range(0, 640, 128):
                g = acc[pl.ds(r, 128), n:n + 128]
                h = g / (1 + jnp.exp(-g)) * acc[pl.ds(r, 128), 640 + n:768 + n]
                hid[pl.ds(r, 128), n:n + 128] = h.astype(BF16)
            m = acc[pl.ds(r, 128), 1280:1408]
            h = m / (1 + jnp.exp(-m)) * swap(m)
            hid[pl.ds(r, 128), 640:768] = jnp.where(low128, h, 0).astype(BF16)

        pl.loop(0, count // 128)(step)

    one, two, last = slice(0, 1), slice(1, 3), slice(3, 4)
    steps = (((one, one),), ((one, two), (two, one)), ((two, two),), ((two, last), (last, two)),
             ((one, last), (last, one), (last, last)))

    def slots_of(parts):
        return [(py, px) for rows, cols in parts for py in range(4)[rows] for px in range(4)[cols]]

    def remote(s, n):
        slots = slots_of(steps[n])
        right = jnp.concatenate([d[:, (py * 4 + px) * 128:(py * 4 + px + 1) * 128] for py, px in slots], axis=1)
        part = jnp.dot(hid[1024 + 512 * s:1536 + 512 * s, :], right, preferred_element_type=F32).astype(BF16)
        for i, (py, px) in enumerate(slots):
            ps[s, py, px] = part[256:512, 128 * i:128 * (i + 1)]
            rp[s, py, px] = part[0:256, 128 * i:128 * (i + 1)]
        for rows, cols in steps[n]:
            remote_copy(ps.at[s, rows, cols], pr.at[s, rows, cols], sent.at[4], pr_r.at[s, n], partner).start()

    def pass_on(s, n):
        slots = slots_of(steps[n])
        arrived(pr.at[s, 0, 0:len(slots)], pr_r.at[s, n])
        for py, px in slots:
            both = (rp[s, py, px].astype(F32) + pr[s, py, px].astype(F32)).astype(BF16)
            zs[s, 0, py, px] = both[0:128]
            zs[s, 1, py, px] = both[128:256]
        for rows, cols in steps[n]:
            for h, way in ((0, -1), (1, 1)):
                remote_copy(zs.at[s, h, rows, cols], zr.at[s, h, rows, cols], sent.at[5], zr_r.at[s], to_z[way]).start()

    norm(0)
    pl.semaphore_wait(barrier, 7)
    zw[0].start()
    zw[1].start()
    send(A, 0, 1, 4, 8)
    tok_z[0].start()
    tok_c[0].start()
    for c in (2, 1, 3):
        norm(c)
        tok_z[c].start()
        tok_c[c].start()

    loads[2].wait()
    loads[3].wait()
    for i in range(11):
        turned = wd[:, i * 128:(i + 1) * 128].astype(F32).T.astype(BF16)
        at = i * 128
        if i < 5:
            dd[0, at:at + 128] = turned
        elif i == 5:
            dd[0, 640:704] = turned[0:64]
            dd[1, 640:704] = turned[64:128]
        else:
            dd[1, at - 768:at - 640] = turned
    zw[2].start()
    zw[3].start()
    d[Q:768, :] = jnp.zeros((64, D), BF16)

    arrived(w.at[0:64], zw_r.at[0])
    send(B, 0, 1, 4, 8)
    recv(A, 0)
    send(A, 2, 3, 5, 9)
    recv(B, 0)
    send(B, 2, 3, 5, 9)
    recv(A, 4)
    send(A, 6, 10, 12, 16)
    recv(B, 4)
    send(B, 6, 10, 12, 16)
    arrived(t.at[:, 0:512], tk_r.at[2])
    recv(A, 2)
    send(A, 7, 11)
    recv(A, 5)
    send(A, 13, 17)
    recv(B, 2)
    send(B, 7, 11)
    here, near, far = (y, 4 + x), ((y + 1) % 4, (y + 3) % 4, 4 + (x + 1) % 4, 4 + (x + 3) % 4), ((y + 2) % 4, 4 + (x + 2) % 4)
    gates(here, 0, 512, True)
    recv(B, 5)
    send(B, 13, 17)
    forward(0)
    gates(here, 512, 512, True)
    recv(A, 6)
    send(A, 14, 18)
    forwarded(0)
    gates(here, 1024, 512, True)
    recv(B, 6)
    send(B, 14, 18)
    recv(A, 7)
    send(A, 15, 19)
    recv(B, 7)
    send(B, 15, 19)
    gates(near, 1024, 512, False)
    forward(1)

    arrived(dz, zw_r.at[1])
    own_half = (lax.broadcasted_iota(jnp.int32, (Q, 128), 1) < 64) == (zlo == 0)
    d[0:Q, 0:128] = jnp.where(own_half, dd[zlo].astype(F32), dz[...].astype(F32)).astype(BF16)
    send(C, 0, 1)
    send(E, 0, 1)
    send(C, 4, 8)
    send(E, 4, 8)
    forwarded(1)
    gates(here + near, 1536, 512, True)
    recv(A, 12)
    recv(B, 12)
    gates(far, 1024, 512, False)
    hide(1024, 512)
    remote(0, 0)
    gates(far, 1536, 512, False)
    pass_on(0, 0)
    hide(1536, 512)
    remote(1, 0)
    recv(C, 0)
    send(C, 2, 3, 5, 9)
    recv(E, 0)
    send(E, 2, 3, 5, 9)
    recv(C, 4)
    send(C, 6, 10, 12, 16)
    recv(E, 4)
    send(E, 6, 10, 12, 16)
    remote(0, 1)
    pass_on(1, 0)
    remote(1, 1)
    pass_on(0, 1)
    recv(C, 2)
    send(C, 7, 11)
    recv(E, 2)
    send(E, 7, 11)
    pass_on(1, 1)
    recv(C, 5)
    send(C, 13, 17)
    recv(E, 5)
    send(E, 13, 17)
    gates(near, 0, 512, False)
    recv(C, 6)
    send(C, 14, 18)
    recv(E, 6)
    send(E, 14, 18)
    remote(0, 2)
    gates(near, 512, 512, False)
    pass_on(0, 2)
    remote(1, 2)
    recv(C, 7)
    send(C, 15, 19)
    recv(E, 7)
    send(E, 15, 19)
    gates(far, 0, 512, False)
    pass_on(1, 2)
    gates(far, 512, 512, False)
    hide(0, 1024)
    recv(C, 12)
    recv(E, 12)
    recv(C, 13)
    recv(E, 13)
    remote(0, 3)
    remote(0, 4)
    pass_on(0, 3)
    remote(1, 3)
    pass_on(0, 4)
    remote(1, 4)
    pass_on(1, 3)

    for n in range(4):
        cols = slice(512 * n, 512 * (n + 1))
        os_[:, cols] = jnp.dot(hid[512:1024, :], d[:, cols], preferred_element_type=F32).astype(BF16)
        remote_copy(os_.at[:, cols], or_.at[:, cols], sent.at[6], or_r.at[0], partner).start()
        place = slice(512 * (n % 2), 512 * (n % 2 + 1))
        acc[1024 + 512 * (n // 2):1536 + 512 * (n // 2), place] = jnp.dot(hid[0:512, :], d[:, cols], preferred_element_type=F32)
        if n == 0:
            pass_on(1, 4)
    arrived(or_, or_r.at[0])

    post = post_ref[...].astype(F32).reshape(1, D)
    low16 = lax.broadcasted_iota(jnp.int32, (16, 128), 1) < 64

    def spot(theirs, me):
        o = (theirs - me + 4) % 4
        return o + o // 2 - o // 3 * 2

    spots = [(spot(j // 4, y), spot(j % 4, x)) for j in range(16)]

    def finish(s, h, i):
        r = pl.multiple_of(i * 16, 16)
        row = pl.multiple_of((2 * h + s) * 128 + r, 16)
        b, square = [], jnp.zeros((16, 128), F32)
        for py, px in spots:
            cols = pl.ds(pl.multiple_of((py * 4 + px) * 128, 128), 128)
            mine = acc[pl.ds(1024 + py // 2 * 512 + row, 16), pl.ds(pl.multiple_of((py % 2 * 4 + px) * 128, 128), 128)]
            v = mine + or_[pl.ds(row, 16), cols].astype(F32)
            b.append((v + zr[s, h, py, px, pl.ds(r, 16), :].astype(F32)).astype(BF16))
            v = b[-1].astype(F32)
            square += v * v
        scale = 0.5 * lax.rsqrt(jnp.sum(square, axis=-1, keepdims=True) * (1 / D) + EPS)
        for j in range(16):
            one, two = b[2 * (j % 8)].astype(F32), b[2 * (j % 8) + 1].astype(F32)
            v = jnp.where(low16, one, swap(two)) if j < 8 else jnp.where(low16, swap(one), two)
            cols = slice(128 * j, 128 * (j + 1))
            v = tok[pl.ds(row, 16), cols].astype(F32) + v * scale * post[:, cols]
            out_ref[pl.ds(row, 16), cols] = v.astype(BF16)

    for s in (0, 1):
        arrived(zr.at[s], zr_r.at[s])
        for h in (0, 1):
            pl.loop(0, 8, unroll=2)(lambda i, s=s, h=h: finish(s, h, i))

    left(w.at[0:1920], sent.at[0])
    left(w.at[0:960], sent.at[1])
    left(w.at[0:128], sent.at[2])
    left(t.at[:, 0:1536], sent.at[3])
    left(ps, sent.at[4])
    left(zs, sent.at[5])
    left(os_, sent.at[6])


def shards(tokens, pre_gain, gate_weight, value_weight, down_weight, post_gain):
    any_, vmem = pl.BlockSpec(memory_space=pl.ANY), pl.BlockSpec(memory_space=pltpu.VMEM)
    sem = pltpu.SemaphoreType.DMA
    buf = lambda *s, t=BF16: pltpu.VMEM(s, t)
    return pl.pallas_call(
        kernel,
        out_shape=pltpu.VMEM((TOK, D), BF16),
        in_specs=[any_, vmem, any_, any_, any_, vmem],
        out_specs=vmem,
        scratch_shapes=[
            buf(TOK, D), buf(64, F), buf(64, F), buf(128, F), buf(2, Q, 128), buf(Q, 128), buf(2112, F), buf(768, D),
            buf(8, 2560, 256), buf(2048, F, t=F32), buf(2048, 768), *[buf(2, 4, 4, 256, 128)] * 3, *[buf(2, 2, 4, 4, 128, 128)] * 2,
            buf(TOK, D), buf(TOK, D),
            sem((8,)), sem((4, 8)), sem((2,)), sem((5,)), sem((2, 5)), sem((2,)), sem((1,)), sem((7,)),
        ],
        compiler_params=pltpu.CompilerParams(collective_id=0, has_side_effects=True, vmem_limit_bytes=61 * 1024 * 1024),
    )(tokens, pre_gain, gate_weight, value_weight, down_weight.T, post_gain)


def solution(mesh):
    rows = P(("rep", "fs", "tp"), None)
    in_specs = (rows, P(), P("fs", "tp"), P("fs", "tp"), P("tp", "fs"), P())
    return jax.shard_map(shards, mesh=mesh, in_specs=in_specs, out_specs=rows, check_vma=False)
```

```python
import jax
import jax.numpy as jnp
from jax import lax
from jax.experimental import pallas as pl
from jax.experimental.pallas import tpu as pltpu
from jax.sharding import PartitionSpec as P

D, F, Q, TOK = 2048, 1408, 704, 512
SENT = 2048
EPS = 1e-06
F32, BF16 = jnp.float32, jnp.bfloat16


def remote_copy(src, dst, send_sem, recv_sem, to):
    return pltpu.make_async_remote_copy(src_ref=src, dst_ref=dst, send_sem=send_sem, recv_sem=recv_sem, device_id=to,
                                        device_id_type=pl.DeviceIdType.MESH)


TOGETHER = {0: (0, 2), 1: (0, 2), 4: (1, 2), 8: (1, 2), 2: (2, 1), 3: (2, 1), 5: (3, 2), 9: (3, 2), 6: (4, 2), 10: (4, 2),
            7: (5, 2), 11: (5, 2)}


def ring_copies(block, half, to_a, to_b, send, recv):
    c = []
    for way in (1, -1):
        c.append((block(0, 0, 0, 0), block(0, 0, way, 0), to_a[way]))
    for way, h in ((1, 0), (-1, 1)):
        c.append((half(-way, 0, 0, 0, h), half(-way, 0, way, 0, h), to_a[way]))
    for way in (1, -1):
        for oa in (0, -1, 1, 2):
            c.append((block(oa, 0, 0, 0), block(oa, 0, 0, way), to_b[way]))
    for way, h in ((1, 0), (-1, 1)):
        for oa in (0, -1, 1, 2):
            c.append((half(oa, -way, 0, 0, h), half(oa, -way, 0, way, h), to_b[way]))
    return [remote_copy(src, dst, send, recv(i), to) for i, (src, dst, to) in enumerate(c)]


def position(offset):
    return (0, 1, 3, 2)[offset % 4]


def kernel(tok_in, pre_ref, gate_in, value_in, down_in, post_ref, out_ref, tok, wg, wv, wd, dd, dz, w, d, t, acc, hid, ps,
           pr, rp, zs, zr, os_, or_, load, ag_r, zw_r, tk_r, pr_r, zr_r, or_r, sent):
    rep, fs, core = lax.axis_index("rep"), lax.axis_index("fs"), lax.axis_index("tp")
    zlo, y, x = fs // 16, (fs // 4) % 4, fs % 4
    z = rep * 2 + zlo

    def device(dz_=0, dy=0, dx=0, other=False):
        zz, yy, xx = (z + dz_ + 4) % 4, (y + dy + 4) % 4, (x + dx + 4) % 4
        return {"rep": zz // 2, "fs": (zz % 2) * 16 + yy * 4 + xx, "tp": 1 - core if other else core}

    to_x = {1: device(dx=1), -1: device(dx=-1)}
    to_y = {1: device(dy=1), -1: device(dy=-1)}
    to_z = {1: device(dz_=1), -1: device(dz_=-1)}
    partner = device(other=True)

    loads = [
        pltpu.make_async_copy(gate_in, wg, load.at[0]),
        pltpu.make_async_copy(value_in, wv, load.at[1]),
        pltpu.make_async_copy(down_in, wd.at[0:64], load.at[2]),
        pltpu.make_async_copy(down_in, wd.at[64:128], load.at[3]),
    ] + [pltpu.make_async_copy(tok_in.at[128 * c:128 * c + 128], tok.at[128 * c:128 * c + 128], load.at[4 + c]) for c in range(4)]
    for c in loads:
        c.start()

    barrier = pltpu.get_barrier_semaphore()
    for peer in (*to_x.values(), *to_y.values(), *to_z.values(), partner):
        pl.semaphore_signal(barrier, inc=1, device_id=peer, device_id_type=pl.DeviceIdType.MESH)

    lanes = lax.broadcasted_iota(jnp.int32, (64, 128), 1)
    low = lanes < 64
    swap = lambda v: pltpu.roll(v, 64, 1)

    loads[0].wait()
    loads[1].wait()
    place = (y * 4 + x) * 64
    for q in (0, 1):
        at = pl.multiple_of(place + (zlo + q) % 2 * (2048 - place), 64)
        g5, v5 = wg[:, 640:768].astype(F32), wv[:, 640:768].astype(F32)
        first = 768 * q
        w[pl.ds(at, 64), 0:640] = wg[:, first:first + 640]
        w[pl.ds(at, 64), 640:1280] = wv[:, first:first + 640]
        mixed = jnp.where(low, g5, swap(v5)) if q == 0 else jnp.where(low, swap(g5), v5)
        w[pl.ds(at, 64), 1280:1408] = mixed.astype(BF16)

    def slot(oy, ox):
        return (y + oy + 4) % 4, (x + ox + 4) % 4

    def gv(first, rows, h):
        def ref(oa, ob, ma, mb):
            yy, xx = slot(ob, oa) if first == "x" else slot(oa, ob)
            at = (yy * 4 + xx) * 64 if first == "x" else 1024 + (xx * 4 + yy) * 64
            return w.at[pl.ds(pl.multiple_of(at + h * rows, rows), rows)]

        return ref

    def dn(first, rows, h):
        def ref(oa, ob, ma, mb):
            oa, ob = position(oa - ma), position(ob - mb)
            at = (0 if first == "x" else 352) + h * rows
            n = (ob * 4 + oa if first == "x" else oa * 4 + ob) * 128
            return d.at[at:at + rows, n:n + 128]

        return ref

    def arrived(ref, sem):
        remote_copy(ref, ref, sem, sem, partner).wait_recv()

    def left(ref, sem):
        remote_copy(ref, ref, sem, sem, partner).wait_send()

    def together(i, kind):
        if i in TOGETHER:
            return TOGETHER[i]
        if kind is gv:
            return 6, 4
        return (6, 1) if i in (12, 16) else (7, 3)

    items = []
    for i, (make, rows, first) in enumerate(((gv, 64, "x"), (gv, 64, "y"), (dn, 352, "x"), (dn, 352, "y"))):
        halves = [make(first, rows // 2, h) for h in (0, 1)]
        half = lambda oa, ob, ma, mb, h, halves=halves: halves[h](oa, ob, ma, mb)
        a, b = (to_x, to_y) if first == "x" else (to_y, to_x)
        sem = lambda n, i=i, make=make: ag_r.at[i, together(n, make)[0]]
        items.append((ring_copies(make(first, rows, 0), half, a, b, sent.at[i // 2], sem), make, i))
    A, B, C, E = items

    def send(item, *which):
        for i in which:
            item[0][i].start()

    def recv(item, which):
        group, blocks = together(which, item[1])
        ref = w.at[0:64 * blocks] if item[1] is gv else d.at[0:352, 0:128 * blocks]
        arrived(ref, ag_r.at[item[2], group])

    def rows_of(ref, at, n):
        return ref.at[pl.ds(pl.multiple_of(at, n), n)]

    zw = []
    for h, way in ((0, 1), (1, -1)):
        dst = rows_of(w, 1024 + (x * 4 + y) * 64 + 32 * h, 32)
        zw.append(remote_copy(w.at[2048 + 32 * h:2080 + 32 * h], dst, sent.at[2], zw_r.at[0], to_z[way]))
    for h, way in ((0, 1), (1, -1)):
        part = pl.ds(352 * h, 352)
        zw.append(remote_copy(dd.at[1 - zlo, part], dz.at[part], sent.at[2], zw_r.at[1], to_z[way]))

    def group_rows(at):
        return t.at[:, pl.ds(at, 128)]

    tok_z, tok_c, tok_f = [], [], []
    for c in range(4):
        r = 128 * c
        mine = 1024 + 512 * (c % 2) + 128 * (c // 2)
        tok_z.append(remote_copy(group_rows(SENT + r), group_rows(mine), sent.at[3], tk_r.at[c % 2], to_z[1 if c < 2 else -1]))
        tok_c.append(remote_copy(group_rows(r), group_rows(512 + r), sent.at[3], tk_r.at[2], partner))
        tok_f.append(remote_copy(group_rows(mine), group_rows(mine + 256), sent.at[3], tk_r.at[3 + c % 2], partner))

    def forward(half):
        arrived(t.at[:, 0:256], tk_r.at[half])
        tok_f[half].start()
        tok_f[half + 2].start()

    def forwarded(half):
        arrived(t.at[:, 0:256], tk_r.at[3 + half])

    gain = pre_ref[...].astype(F32).reshape(1, D)
    low32 = lax.broadcasted_iota(jnp.int32, (32, 128), 1) < 64

    def norm_rows(r):
        v = tok[pl.ds(r, 32), :].astype(F32)
        v = v * lax.rsqrt(jnp.mean(v * v, axis=-1, keepdims=True) + EPS) * gain
        for k in (0, 1):
            straight = pl.multiple_of((zlo + k) % 2 * SENT + r, 32)
            turned = pl.multiple_of((zlo + k + 1) % 2 * SENT + r, 32)
            tiles = [v[:, k * 1024 + 128 * i:k * 1024 + 128 * (i + 1)] for i in range(8)]
            flipped = [swap(s) for s in tiles]
            for i in range(8):
                t[i // 2, pl.ds(straight, 32), 128 * (i % 2):128 * (i % 2 + 1)] = tiles[i].astype(BF16)
            for xx in range(4):
                for p in (0, 1):
                    one, two = 4 * p + xx // 2, 4 * p + 2 + xx // 2
                    if xx % 2 == 0:
                        out = jnp.where(low32, tiles[one], flipped[two])
                    else:
                        out = jnp.where(low32, flipped[one], tiles[two])
                    t[4 + xx, pl.ds(turned, 32), 128 * p:128 * (p + 1)] = out.astype(BF16)

    def norm(c):
        loads[4 + c].wait()
        pl.loop(0, 4)(lambda i: norm_rows(pl.multiple_of(c * 128 + i * 32, 32)))

    def gates(groups, row, count, first):
        for n in range(0, F, 256):
            m = min(256, F - n)
            total = None if first else acc[row:row + count, n:n + m]
            for g in groups:
                part = jnp.dot(t[g, row:row + count, :], w[pl.ds(pl.multiple_of(g * 256, 256), 256), n:n + m],
                               preferred_element_type=F32)
                total = part if total is None else total + part
            acc[row:row + count, n:n + m] = total

    low128 = lax.broadcasted_iota(jnp.int32, (128, 128), 1) < 64

    def hide(row, count):
        def step(i):
            r = pl.multiple_of(row + i * 128, 128)
            for n in range(0, 640, 128):
                g = acc[pl.ds(r, 128), n:n + 128]
                h = g / (1 + jnp.exp(-g)) * acc[pl.ds(r, 128), 640 + n:768 + n]
                hid[pl.ds(r, 128), n:n + 128] = h.astype(BF16)
            m = acc[pl.ds(r, 128), 1280:1408]
            h = m / (1 + jnp.exp(-m)) * swap(m)
            hid[pl.ds(r, 128), 640:768] = jnp.where(low128, h, 0).astype(BF16)

        pl.loop(0, count // 128)(step)

    one, two, last = slice(0, 1), slice(1, 3), slice(3, 4)
    steps = (((one, one),), ((one, two), (two, one)), ((two, two),), ((one, last), (last, one)),
             ((two, last), (last, two), (last, last)))

    def slots_of(parts):
        return [(py, px) for rows, cols in parts for py in range(4)[rows] for px in range(4)[cols]]

    def remote(s, n):
        slots = slots_of(steps[n])
        right = jnp.concatenate([d[:, (py * 4 + px) * 128:(py * 4 + px + 1) * 128] for py, px in slots], axis=1)
        part = jnp.dot(hid[1024 + 512 * s:1536 + 512 * s, :], right, preferred_element_type=F32).astype(BF16)
        for i, (py, px) in enumerate(slots):
            ps[s, py, px] = part[256:512, 128 * i:128 * (i + 1)]
            rp[s, py, px] = part[0:256, 128 * i:128 * (i + 1)]
        for rows, cols in steps[n]:
            remote_copy(ps.at[s, rows, cols], pr.at[s, rows, cols], sent.at[4], pr_r.at[s, n], partner).start()

    def pass_on(s, n):
        slots = slots_of(steps[n])
        arrived(pr.at[s, :, 0] if len(slots) == 4 else d.at[0:256, 0:128 * len(slots)], pr_r.at[s, n])
        for py, px in slots:
            both = (rp[s, py, px].astype(F32) + pr[s, py, px].astype(F32)).astype(BF16)
            zs[s, 0, py, px] = both[0:128]
            zs[s, 1, py, px] = both[128:256]
        for rows, cols in steps[n]:
            for h, way in ((0, -1), (1, 1)):
                remote_copy(zs.at[s, h, rows, cols], zr.at[s, h, rows, cols], sent.at[5], zr_r.at[s], to_z[way]).start()

    norm(0)
    pl.semaphore_wait(barrier, 7)
    zw[0].start()
    zw[1].start()
    send(A, 0, 1, 4, 8)
    tok_c[0].start()
    for c in (2, 1, 3):
        norm(c)
        if c == 2:
            tok_z[0].start()
        tok_z[c].start()
        tok_c[c].start()

    loads[2].wait()
    loads[3].wait()
    for i in range(11):
        turned = wd[:, i * 128:(i + 1) * 128].astype(F32).T.astype(BF16)
        at = i * 128
        if i < 5:
            dd[0, at:at + 128] = turned
        elif i == 5:
            dd[0, 640:704] = turned[0:64]
            dd[1, 640:704] = turned[64:128]
        else:
            dd[1, at - 768:at - 640] = turned
    zw[2].start()
    zw[3].start()
    d[Q:768, :] = jnp.zeros((64, D), BF16)

    arrived(w.at[0:64], zw_r.at[0])
    send(B, 0, 1, 4, 8)
    recv(A, 0)
    send(A, 2, 3, 5, 9)
    recv(B, 0)
    send(B, 2, 3, 5, 9)
    recv(A, 4)
    send(A, 6, 10, 12, 16)
    recv(B, 4)
    send(B, 6, 10, 12, 16)
    arrived(t.at[:, 0:512], tk_r.at[2])
    recv(A, 2)
    send(A, 7, 11)
    recv(A, 5)
    send(A, 13, 17)
    recv(B, 2)
    send(B, 7, 11)
    here, near, far = (y, 4 + x), ((y + 1) % 4, (y + 3) % 4, 4 + (x + 1) % 4, 4 + (x + 3) % 4), ((y + 2) % 4, 4 + (x + 2) % 4)
    gates(here, 0, 512, True)
    recv(B, 5)
    send(B, 13, 17)
    forward(0)
    gates(here, 512, 512, True)
    recv(A, 6)
    send(A, 14, 18)
    forwarded(0)
    gates(here, 1024, 512, True)
    recv(B, 6)
    send(B, 14, 18)
    recv(A, 7)
    send(A, 15, 19)
    recv(B, 7)
    send(B, 15, 19)
    forward(1)
    gates(near, 1024, 512, False)

    arrived(dz, zw_r.at[1])
    own_half = (lax.broadcasted_iota(jnp.int32, (Q, 128), 1) < 64) == (zlo == 0)
    d[0:Q, 0:128] = jnp.where(own_half, dd[zlo].astype(F32), dz[...].astype(F32)).astype(BF16)
    send(C, 0, 1)
    send(E, 0, 1)
    send(C, 4, 8)
    send(E, 4, 8)
    gates(here + near, 1536, 256, True)
    forwarded(1)
    gates(here + near, 1792, 256, True)
    recv(A, 12)
    recv(B, 12)
    gates(far, 1024, 512, False)
    hide(1024, 512)
    remote(0, 0)
    recv(C, 0)
    send(C, 2, 3, 5, 9)
    recv(E, 0)
    send(E, 2, 3, 5, 9)
    recv(C, 4)
    send(C, 6, 10, 12, 16)
    recv(E, 4)
    send(E, 6, 10, 12, 16)
    remote(0, 1)
    gates(far, 1536, 512, False)
    pass_on(0, 0)
    pass_on(0, 1)
    hide(1536, 512)
    remote(1, 0)
    remote(1, 1)
    recv(C, 2)
    send(C, 7, 11)
    recv(E, 2)
    send(E, 7, 11)
    pass_on(1, 0)
    pass_on(1, 1)
    recv(C, 5)
    send(C, 13, 17)
    recv(E, 5)
    send(E, 13, 17)
    recv(C, 6)
    send(C, 14, 18)
    recv(E, 6)
    send(E, 14, 18)
    remote(0, 2)
    remote(1, 2)
    gates(near, 0, 512, False)
    pass_on(0, 2)
    pass_on(1, 2)
    recv(C, 7)
    send(C, 15, 19)
    recv(E, 7)
    send(E, 15, 19)
    recv(C, 12)
    recv(E, 12)
    remote(0, 3)
    remote(1, 3)
    gates(near, 512, 512, False)
    pass_on(0, 3)
    pass_on(1, 3)
    gates(far, 0, 512, False)
    recv(C, 13)
    recv(E, 13)
    remote(0, 4)
    remote(1, 4)
    gates(far, 512, 512, False)
    pass_on(0, 4)
    pass_on(1, 4)
    hide(0, 1024)

    for n in range(4):
        cols = slice(512 * n, 512 * (n + 1))
        os_[:, cols] = jnp.dot(hid[512:1024, :], d[:, cols], preferred_element_type=F32).astype(BF16)
        remote_copy(os_.at[:, cols], or_.at[:, cols], sent.at[6], or_r.at[0], partner).start()
        place = slice(512 * (n % 2), 512 * (n % 2 + 1))
        acc[1024 + 512 * (n // 2):1536 + 512 * (n // 2), place] = jnp.dot(hid[0:512, :], d[:, cols], preferred_element_type=F32)
    arrived(or_, or_r.at[0])

    post = post_ref[...].astype(F32).reshape(1, D)
    low16 = lax.broadcasted_iota(jnp.int32, (16, 128), 1) < 64

    def spot(theirs, me):
        o = (theirs - me + 4) % 4
        return o + o // 2 - o // 3 * 2

    spots = [(spot(j // 4, y), spot(j % 4, x)) for j in range(16)]

    def finish(s, h, i):
        r = pl.multiple_of(i * 16, 16)
        row = pl.multiple_of((2 * h + s) * 128 + r, 16)
        b, square = [], jnp.zeros((16, 128), F32)
        for py, px in spots:
            cols = pl.ds(pl.multiple_of((py * 4 + px) * 128, 128), 128)
            mine = acc[pl.ds(1024 + py // 2 * 512 + row, 16), pl.ds(pl.multiple_of((py % 2 * 4 + px) * 128, 128), 128)]
            v = mine + or_[pl.ds(row, 16), cols].astype(F32)
            b.append((v + zr[s, h, py, px, pl.ds(r, 16), :].astype(F32)).astype(BF16))
            v = b[-1].astype(F32)
            square += v * v
        scale = 0.5 * lax.rsqrt(jnp.sum(square, axis=-1, keepdims=True) * (1 / D) + EPS)
        for j in range(16):
            one, two = b[2 * (j % 8)].astype(F32), b[2 * (j % 8) + 1].astype(F32)
            v = jnp.where(low16, one, swap(two)) if j < 8 else jnp.where(low16, swap(one), two)
            cols = slice(128 * j, 128 * (j + 1))
            v = tok[pl.ds(row, 16), cols].astype(F32) + v * scale * post[:, cols]
            out_ref[pl.ds(row, 16), cols] = v.astype(BF16)

    for s in (0, 1):
        arrived(zr.at[s], zr_r.at[s])
        for h in (0, 1):
            pl.loop(0, 8, unroll=2)(lambda i, s=s, h=h: finish(s, h, i))

    left(w.at[0:1920], sent.at[0])
    left(w.at[0:960], sent.at[1])
    left(w.at[0:128], sent.at[2])
    left(t.at[:, 0:1536], sent.at[3])
    left(ps, sent.at[4])
    left(zs, sent.at[5])
    left(os_, sent.at[6])


def shards(tokens, pre_gain, gate_weight, value_weight, down_weight, post_gain):
    any_, vmem = pl.BlockSpec(memory_space=pl.ANY), pl.BlockSpec(memory_space=pltpu.VMEM)
    sem = pltpu.SemaphoreType.DMA
    buf = lambda *s, t=BF16: pltpu.VMEM(s, t)
    return pl.pallas_call(
        kernel,
        out_shape=pltpu.VMEM((TOK, D), BF16),
        in_specs=[any_, vmem, any_, any_, any_, vmem],
        out_specs=vmem,
        scratch_shapes=[
            buf(TOK, D), buf(64, F), buf(64, F), buf(128, F), buf(2, Q, 128), buf(Q, 128), buf(2112, F), buf(768, D),
            buf(8, 2560, 256), buf(2048, F, t=F32), buf(2048, 768), *[buf(2, 4, 4, 256, 128)] * 3, *[buf(2, 2, 4, 4, 128, 128)] * 2,
            buf(TOK, D), buf(TOK, D),
            sem((8,)), sem((4, 8)), sem((2,)), sem((5,)), sem((2, 5)), sem((2,)), sem((1,)), sem((7,)),
        ],
        compiler_params=pltpu.CompilerParams(collective_id=0, has_side_effects=True, vmem_limit_bytes=61 * 1024 * 1024),
    )(tokens, pre_gain, gate_weight, value_weight, down_weight.T, post_gain)


def solution(mesh):
    rows = P(("rep", "fs", "tp"), None)
    in_specs = (rows, P(), P("fs", "tp"), P("fs", "tp"), P("tp", "fs"), P())
    return jax.shard_map(shards, mesh=mesh, in_specs=in_specs, out_specs=rows, check_vma=False)
```

```python
import jax
import jax.numpy as jnp
from jax import lax
from jax.experimental import pallas as pl
from jax.experimental.pallas import tpu as pltpu
from jax.sharding import PartitionSpec as P

D, F, Q, TOK = 2048, 1408, 704, 512
SENT = 2048
EPS = 1e-06
F32, BF16 = jnp.float32, jnp.bfloat16


def remote_copy(src, dst, send_sem, recv_sem, to):
    return pltpu.make_async_remote_copy(src_ref=src, dst_ref=dst, send_sem=send_sem, recv_sem=recv_sem, device_id=to,
                                        device_id_type=pl.DeviceIdType.MESH)


TOGETHER = {0: (0, 2), 1: (0, 2), 4: (1, 2), 8: (1, 2), 2: (2, 1), 3: (2, 1), 5: (3, 2), 9: (3, 2), 6: (4, 2), 10: (4, 2),
            7: (5, 2), 11: (5, 2)}


def ring_copies(block, half, to_a, to_b, send, recv):
    c = []
    for way in (1, -1):
        c.append((block(0, 0, 0, 0), block(0, 0, way, 0), to_a[way]))
    for way, h in ((1, 0), (-1, 1)):
        c.append((half(-way, 0, 0, 0, h), half(-way, 0, way, 0, h), to_a[way]))
    for way in (1, -1):
        for oa in (0, -1, 1, 2):
            c.append((block(oa, 0, 0, 0), block(oa, 0, 0, way), to_b[way]))
    for way, h in ((1, 0), (-1, 1)):
        for oa in (0, -1, 1, 2):
            c.append((half(oa, -way, 0, 0, h), half(oa, -way, 0, way, h), to_b[way]))
    return [remote_copy(src, dst, send, recv(i), to) for i, (src, dst, to) in enumerate(c)]


def position(offset):
    return (0, 1, 3, 2)[offset % 4]


def kernel(tok_in, pre_ref, gate_in, value_in, down_in, post_ref, out_ref, tok, wg, wv, wd, dd, dz, w, d, t, acc, hid, ps,
           pr, rp, zs, zr, os_, or_, squares, load, ag_r, zw_r, tk_r, pr_r, zr_r, or_r, sent):
    rep, fs, core = lax.axis_index("rep"), lax.axis_index("fs"), lax.axis_index("tp")
    zlo, y, x = fs // 16, (fs // 4) % 4, fs % 4
    z = rep * 2 + zlo

    def device(dz_=0, dy=0, dx=0, other=False):
        zz, yy, xx = (z + dz_ + 4) % 4, (y + dy + 4) % 4, (x + dx + 4) % 4
        return {"rep": zz // 2, "fs": (zz % 2) * 16 + yy * 4 + xx, "tp": 1 - core if other else core}

    to_x = {1: device(dx=1), -1: device(dx=-1)}
    to_y = {1: device(dy=1), -1: device(dy=-1)}
    to_z = {1: device(dz_=1), -1: device(dz_=-1)}
    partner = device(other=True)

    loads = [
        pltpu.make_async_copy(gate_in, wg, load.at[0]),
        pltpu.make_async_copy(value_in, wv, load.at[1]),
        pltpu.make_async_copy(down_in, wd.at[0:64], load.at[2]),
        pltpu.make_async_copy(down_in, wd.at[64:128], load.at[3]),
    ] + [pltpu.make_async_copy(tok_in.at[128 * c:128 * c + 128], tok.at[128 * c:128 * c + 128], load.at[4 + c]) for c in range(4)]
    barrier = pltpu.get_barrier_semaphore()
    for peer in (*to_x.values(), *to_y.values(), *to_z.values(), partner):
        pl.semaphore_signal(barrier, inc=1, device_id=peer, device_id_type=pl.DeviceIdType.MESH)

    for c in loads:
        c.start()

    lanes = lax.broadcasted_iota(jnp.int32, (64, 128), 1)
    low = lanes < 64
    swap = lambda v: pltpu.roll(v, 64, 1)

    loads[0].wait()
    loads[1].wait()
    place = (y * 4 + x) * 64
    for q in (0, 1):
        at = pl.multiple_of(place + (zlo + q) % 2 * (2048 - place), 64)
        g5, v5 = wg[:, 640:768].astype(F32), wv[:, 640:768].astype(F32)
        first = 768 * q
        w[pl.ds(at, 64), 0:640] = wg[:, first:first + 640]
        w[pl.ds(at, 64), 640:1280] = wv[:, first:first + 640]
        mixed = jnp.where(low, g5, swap(v5)) if q == 0 else jnp.where(low, swap(g5), v5)
        w[pl.ds(at, 64), 1280:1408] = mixed.astype(BF16)

    def slot(oy, ox):
        return (y + oy + 4) % 4, (x + ox + 4) % 4

    def gv(first, rows, h):
        def ref(oa, ob, ma, mb):
            yy, xx = slot(ob, oa) if first == "x" else slot(oa, ob)
            at = (yy * 4 + xx) * 64 if first == "x" else 1024 + (xx * 4 + yy) * 64
            return w.at[pl.ds(pl.multiple_of(at + h * rows, rows), rows)]

        return ref

    def dn(first, rows, h):
        def ref(oa, ob, ma, mb):
            oa, ob = position(oa - ma), position(ob - mb)
            at = (0 if first == "x" else 352) + h * rows
            n = (ob * 4 + oa if first == "x" else oa * 4 + ob) * 128
            return d.at[at:at + rows, n:n + 128]

        return ref

    def arrived(ref, sem):
        remote_copy(ref, ref, sem, sem, partner).wait_recv()

    def left(ref, sem):
        remote_copy(ref, ref, sem, sem, partner).wait_send()

    def together(i, kind):
        if i in TOGETHER:
            return TOGETHER[i]
        if kind is gv:
            return 6, 4
        return (6, 1) if i in (12, 16) else (7, 3)

    items = []
    for i, (make, rows, first) in enumerate(((gv, 64, "x"), (gv, 64, "y"), (dn, 352, "x"), (dn, 352, "y"))):
        halves = [make(first, rows // 2, h) for h in (0, 1)]
        half = lambda oa, ob, ma, mb, h, halves=halves: halves[h](oa, ob, ma, mb)
        a, b = (to_x, to_y) if first == "x" else (to_y, to_x)
        sem = lambda n, i=i, make=make: ag_r.at[i, together(n, make)[0]]
        items.append((ring_copies(make(first, rows, 0), half, a, b, sent.at[i // 2], sem), make, i))
    A, B, C, E = items

    def send(item, *which):
        for i in which:
            item[0][i].start()

    def recv(item, which):
        group, blocks = together(which, item[1])
        ref = w.at[0:64 * blocks] if item[1] is gv else d.at[0:352, 0:128 * blocks]
        arrived(ref, ag_r.at[item[2], group])

    def rows_of(ref, at, n):
        return ref.at[pl.ds(pl.multiple_of(at, n), n)]

    zw = []
    for h, way in ((0, 1), (1, -1)):
        dst = rows_of(w, 1024 + (x * 4 + y) * 64 + 32 * h, 32)
        zw.append(remote_copy(w.at[2048 + 32 * h:2080 + 32 * h], dst, sent.at[2], zw_r.at[0], to_z[way]))
    for h, way in ((0, 1), (1, -1)):
        part = pl.ds(352 * h, 352)
        zw.append(remote_copy(dd.at[1 - zlo, part], dz.at[part], sent.at[2], zw_r.at[1], to_z[way]))

    def group_rows(at):
        return t.at[:, pl.ds(at, 128)]

    tok_z, tok_c, tok_f = [], [], []
    for c in range(4):
        r = 128 * c
        mine = 1024 + 512 * (c % 2) + 128 * (c // 2)
        tok_z.append(remote_copy(group_rows(SENT + r), group_rows(mine), sent.at[3], tk_r.at[c % 2], to_z[1 if c < 2 else -1]))
        tok_c.append(remote_copy(group_rows(r), group_rows(512 + r), sent.at[3], tk_r.at[2], partner))
        tok_f.append(remote_copy(group_rows(mine), group_rows(mine + 256), sent.at[3], tk_r.at[3 + c % 2], partner))

    def forward(half):
        arrived(t.at[:, 0:256], tk_r.at[half])
        tok_f[half].start()
        tok_f[half + 2].start()

    def forwarded(half):
        arrived(t.at[:, 0:256], tk_r.at[3 + half])

    gain = pre_ref[...].astype(F32).reshape(1, D)
    low32 = lax.broadcasted_iota(jnp.int32, (32, 128), 1) < 64

    def norm_rows(r):
        v = tok[pl.ds(r, 32), :].astype(F32)
        v = v * lax.rsqrt(jnp.mean(v * v, axis=-1, keepdims=True) + EPS) * gain
        for k in (0, 1):
            straight = pl.multiple_of((zlo + k) % 2 * SENT + r, 32)
            turned = pl.multiple_of((zlo + k + 1) % 2 * SENT + r, 32)
            tiles = [v[:, k * 1024 + 128 * i:k * 1024 + 128 * (i + 1)] for i in range(8)]
            flipped = [swap(s) for s in tiles]
            for i in range(8):
                t[i // 2, pl.ds(straight, 32), 128 * (i % 2):128 * (i % 2 + 1)] = tiles[i].astype(BF16)
            for xx in range(4):
                for p in (0, 1):
                    one, two = 4 * p + xx // 2, 4 * p + 2 + xx // 2
                    if xx % 2 == 0:
                        out = jnp.where(low32, tiles[one], flipped[two])
                    else:
                        out = jnp.where(low32, flipped[one], tiles[two])
                    t[4 + xx, pl.ds(turned, 32), 128 * p:128 * (p + 1)] = out.astype(BF16)

    def norm(c):
        loads[4 + c].wait()
        pl.loop(0, 4)(lambda i: norm_rows(pl.multiple_of(c * 128 + i * 32, 32)))

    def gates(groups, row, count, first):
        for n in range(0, F, 256):
            m = min(256, F - n)
            total = None if first else acc[row:row + count, n:n + m]
            for g in groups:
                part = jnp.dot(t[g, row:row + count, :], w[pl.ds(pl.multiple_of(g * 256, 256), 256), n:n + m],
                               preferred_element_type=F32)
                total = part if total is None else total + part
            acc[row:row + count, n:n + m] = total

    low128 = lax.broadcasted_iota(jnp.int32, (128, 128), 1) < 64

    def hide(row, count):
        def step(i):
            r = pl.multiple_of(row + i * 128, 128)
            for n in range(0, 640, 128):
                g = acc[pl.ds(r, 128), n:n + 128]
                h = g / (1 + jnp.exp(-g)) * acc[pl.ds(r, 128), 640 + n:768 + n]
                hid[pl.ds(r, 128), n:n + 128] = h.astype(BF16)
            m = acc[pl.ds(r, 128), 1280:1408]
            h = m / (1 + jnp.exp(-m)) * swap(m)
            hid[pl.ds(r, 128), 640:768] = jnp.where(low128, h, 0).astype(BF16)

        pl.loop(0, count // 128)(step)

    one, two, last = slice(0, 1), slice(1, 3), slice(3, 4)
    steps = (((one, one),), ((one, two), (two, one)), ((two, two),), ((one, last), (last, one)),
             ((two, last), (last, two), (last, last)))

    def slots_of(parts):
        return [(py, px) for rows, cols in parts for py in range(4)[rows] for px in range(4)[cols]]

    def remote(s, n):
        slots = slots_of(steps[n])
        right = jnp.concatenate([d[:, (py * 4 + px) * 128:(py * 4 + px + 1) * 128] for py, px in slots], axis=1)
        part = jnp.dot(hid[1024 + 512 * s:1536 + 512 * s, :], right, preferred_element_type=F32).astype(BF16)
        for i, (py, px) in enumerate(slots):
            ps[s, py, px] = part[256:512, 128 * i:128 * (i + 1)]
            rp[s, py, px] = part[0:256, 128 * i:128 * (i + 1)]
        for rows, cols in steps[n]:
            remote_copy(ps.at[s, rows, cols], pr.at[s, rows, cols], sent.at[4], pr_r.at[s, n], partner).start()

    def pass_on(s, n):
        slots = slots_of(steps[n])
        arrived(pr.at[s, :, 0] if len(slots) == 4 else d.at[0:256, 0:128 * len(slots)], pr_r.at[s, n])
        for py, px in slots:
            both = (rp[s, py, px].astype(F32) + pr[s, py, px].astype(F32)).astype(BF16)
            zs[s, 0, py, px] = both[0:128]
            zs[s, 1, py, px] = both[128:256]
        for rows, cols in steps[n]:
            for h, way in ((0, -1), (1, 1)):
                remote_copy(zs.at[s, h, rows, cols], zr.at[s, h, rows, cols], sent.at[5], zr_r.at[s, n // 4], to_z[way]).start()

    norm(0)
    pl.semaphore_wait(barrier, 7)
    zw[0].start()
    zw[1].start()
    send(A, 0, 1, 4, 8)
    tok_c[0].start()
    for c in (2, 1, 3):
        norm(c)
        if c == 2:
            tok_z[0].start()
        tok_z[c].start()
        tok_c[c].start()

    loads[2].wait()
    loads[3].wait()
    for i in range(11):
        turned = wd[:, i * 128:(i + 1) * 128].astype(F32).T.astype(BF16)
        at = i * 128
        if i < 5:
            dd[0, at:at + 128] = turned
        elif i == 5:
            dd[0, 640:704] = turned[0:64]
            dd[1, 640:704] = turned[64:128]
        else:
            dd[1, at - 768:at - 640] = turned
    zw[2].start()
    zw[3].start()
    d[Q:768, :] = jnp.zeros((64, D), BF16)

    arrived(w.at[0:64], zw_r.at[0])
    send(B, 0, 1, 4, 8)
    recv(A, 0)
    send(A, 2, 3, 5, 9)
    recv(B, 0)
    send(B, 2, 3, 5, 9)
    recv(A, 4)
    send(A, 6, 10, 12, 16)
    recv(B, 4)
    send(B, 6, 10, 12, 16)
    arrived(t.at[:, 0:512], tk_r.at[2])
    recv(A, 2)
    send(A, 7, 11)
    recv(A, 5)
    send(A, 13, 17)
    recv(B, 2)
    send(B, 7, 11)
    here, near, far = (y, 4 + x), ((y + 1) % 4, (y + 3) % 4, 4 + (x + 1) % 4, 4 + (x + 3) % 4), ((y + 2) % 4, 4 + (x + 2) % 4)
    gates(here, 0, 512, True)
    recv(B, 5)
    send(B, 13, 17)
    forward(0)
    gates(here, 512, 512, True)
    recv(A, 6)
    send(A, 14, 18)
    forwarded(0)
    gates(here, 1024, 512, True)
    recv(B, 6)
    send(B, 14, 18)
    recv(A, 7)
    send(A, 15, 19)
    recv(B, 7)
    send(B, 15, 19)
    forward(1)
    gates(near, 1024, 512, False)

    arrived(dz, zw_r.at[1])
    own_half = (lax.broadcasted_iota(jnp.int32, (Q, 128), 1) < 64) == (zlo == 0)
    d[0:Q, 0:128] = jnp.where(own_half, dd[zlo].astype(F32), dz[...].astype(F32)).astype(BF16)
    send(C, 0, 1)
    send(E, 0, 1)
    send(C, 4, 8)
    send(E, 4, 8)
    gates(here + near, 1536, 256, True)
    forwarded(1)
    gates(here + near, 1792, 256, True)
    recv(A, 12)
    recv(B, 12)
    gates(far, 1024, 512, False)
    hide(1024, 512)
    remote(0, 0)
    recv(C, 0)
    send(C, 2, 3, 5, 9)
    recv(E, 0)
    send(E, 2, 3, 5, 9)
    recv(C, 4)
    send(C, 6, 10, 12, 16)
    recv(E, 4)
    send(E, 6, 10, 12, 16)
    remote(0, 1)
    pass_on(0, 0)
    gates(far, 1536, 512, False)
    pass_on(0, 1)
    hide(1536, 512)
    remote(1, 0)
    remote(1, 1)
    recv(C, 2)
    send(C, 7, 11)
    recv(E, 2)
    send(E, 7, 11)
    pass_on(1, 0)
    pass_on(1, 1)
    recv(C, 5)
    send(C, 13, 17)
    recv(E, 5)
    send(E, 13, 17)
    recv(C, 6)
    send(C, 14, 18)
    recv(E, 6)
    send(E, 14, 18)
    remote(0, 2)
    remote(1, 2)
    pass_on(0, 2)
    pass_on(1, 2)
    gates(near, 0, 512, False)
    recv(C, 7)
    send(C, 15, 19)
    recv(E, 7)
    send(E, 15, 19)
    recv(C, 12)
    recv(E, 12)
    remote(0, 3)
    remote(1, 3)
    gates(far, 512, 512, False)
    pass_on(0, 3)
    pass_on(1, 3)
    gates(far, 0, 512, False)
    recv(C, 13)
    recv(E, 13)
    remote(0, 4)
    remote(1, 4)
    pass_on(0, 4)
    gates(near, 512, 512, False)
    pass_on(1, 4)
    hide(0, 1024)

    for n in range(4):
        cols = slice(512 * n, 512 * (n + 1))
        os_[:, cols] = jnp.dot(hid[512:1024, :], d[:, cols], preferred_element_type=F32).astype(BF16)
        remote_copy(os_.at[:, cols], or_.at[:, cols], sent.at[6], or_r.at[0], partner).start()
    for n in range(4):
        place = slice(512 * (n % 2), 512 * (n % 2 + 1))
        part = jnp.dot(hid[0:512, :], d[:, 512 * n:512 * (n + 1)], preferred_element_type=F32)
        acc[1024 + 512 * (n // 2):1536 + 512 * (n // 2), place] = part
    arrived(or_, or_r.at[0])

    post = post_ref[...].astype(F32).reshape(1, D)
    low16 = lax.broadcasted_iota(jnp.int32, (16, 128), 1) < 64

    def spot(theirs, me):
        o = (theirs - me + 4) % 4
        return o + o // 2 - o // 3 * 2

    spots = [(spot(j // 4, y), spot(j % 4, x)) for j in range(16)]

    early, late = slots_of(sum(steps[:4], ())), slots_of(steps[4])

    def mine(row, py, px):
        return acc.at[pl.ds(pl.multiple_of(1024 + py // 2 * 512 + row, 16), 16), (py % 2 * 4 + px) * 128:(py % 2 * 4 + px + 1) * 128]

    def theirs(row, py, px):
        return or_.at[pl.ds(row, 16), (py * 4 + px) * 128:(py * 4 + px + 1) * 128]

    def places(s, h, i):
        r = pl.multiple_of(i * 16, 16)
        return r, pl.multiple_of((2 * h + s) * 128 + r, 16)

    def prepare(s, h, i):
        r, row = places(s, h, i)
        square = jnp.zeros((16, 128), F32)
        for py, px in early:
            v = mine(row, py, px)[...] + theirs(row, py, px)[...].astype(F32)
            v = (v + zr[s, h, py, px, pl.ds(r, 16), :].astype(F32)).astype(BF16)
            theirs(row, py, px)[...] = v
            square += v.astype(F32) * v.astype(F32)
        for py, px in late:
            mine(row, py, px)[...] += theirs(row, py, px)[...].astype(F32)
        squares[pl.ds(row, 16), :] = square

    def finish(s, h, i):
        r, row = places(s, h, i)
        square = squares[pl.ds(row, 16), :]
        for py, px in late:
            v = (mine(row, py, px)[...] + zr[s, h, py, px, pl.ds(r, 16), :].astype(F32)).astype(BF16)
            theirs(row, py, px)[...] = v
            square += v.astype(F32) * v.astype(F32)
        squares[pl.ds(row, 16), :] = square

    def scales(s, h, i):
        r, row = places(s, h, i)
        mean = jnp.sum(squares[pl.ds(row, 16), :], axis=-1, keepdims=True) * (1 / D)
        squares[pl.ds(row, 16), :] = jnp.broadcast_to(0.5 * lax.rsqrt(mean + EPS), (16, 128))

    def write(s, h, i):
        r, row = places(s, h, i)
        scale = squares[pl.ds(row, 16), :]
        b = []
        for py, px in spots:
            b.append(or_[pl.ds(row, 16), pl.ds(pl.multiple_of((py * 4 + px) * 128, 128), 128)].astype(F32))
        for j in range(16):
            one, two = b[2 * (j % 8)], b[2 * (j % 8) + 1]
            v = jnp.where(low16, one, swap(two)) if j < 8 else jnp.where(low16, swap(one), two)
            cols = slice(128 * j, 128 * (j + 1))
            v = tok[pl.ds(row, 16), cols].astype(F32) + v * scale * post[:, cols]
            out_ref[pl.ds(row, 16), cols] = v.astype(BF16)

    for s in (0, 1):
        arrived(d.at[0:176], zr_r.at[s, 0])
        for h in (0, 1):
            pl.loop(0, 8, unroll=2)(lambda i, s=s, h=h: prepare(s, h, i))
    for s in (0, 1):
        arrived(d.at[0:80], zr_r.at[s, 1])
        for h in (0, 1):
            pl.loop(0, 8, unroll=4)(lambda i, s=s, h=h: finish(s, h, i))
        for h in (0, 1):
            pl.loop(0, 8, unroll=8)(lambda i, s=s, h=h: scales(s, h, i))
        for h in (0, 1):
            pl.loop(0, 8, unroll=2)(lambda i, s=s, h=h: write(s, h, i))

    left(w.at[0:1920], sent.at[0])
    left(w.at[0:960], sent.at[1])
    left(w.at[0:128], sent.at[2])
    left(t.at[:, 0:1536], sent.at[3])
    left(ps, sent.at[4])
    left(zs, sent.at[5])
    left(os_, sent.at[6])


def shards(tokens, pre_gain, gate_weight, value_weight, down_weight, post_gain):
    any_, vmem = pl.BlockSpec(memory_space=pl.ANY), pl.BlockSpec(memory_space=pltpu.VMEM)
    sem = pltpu.SemaphoreType.DMA
    buf = lambda *s, t=BF16: pltpu.VMEM(s, t)
    return pl.pallas_call(
        kernel,
        out_shape=pltpu.VMEM((TOK, D), BF16),
        in_specs=[any_, vmem, any_, any_, any_, vmem],
        out_specs=vmem,
        scratch_shapes=[
            buf(TOK, D), buf(64, F), buf(64, F), buf(128, F), buf(2, Q, 128), buf(Q, 128), buf(2112, F), buf(768, D),
            buf(8, 2560, 256), buf(2048, F, t=F32), buf(2048, 768), *[buf(2, 4, 4, 256, 128)] * 3, *[buf(2, 2, 4, 4, 128, 128)] * 2,
            buf(TOK, D), buf(TOK, D), buf(TOK, 128, t=F32),
            sem((8,)), sem((4, 8)), sem((2,)), sem((5,)), sem((2, 5)), sem((2, 2)), sem((1,)), sem((7,)),
        ],
        compiler_params=pltpu.CompilerParams(collective_id=0, has_side_effects=True, vmem_limit_bytes=61 * 1024 * 1024),
    )(tokens, pre_gain, gate_weight, value_weight, down_weight.T, post_gain)


def solution(mesh):
    rows = P(("rep", "fs", "tp"), None)
    in_specs = (rows, P(), P("fs", "tp"), P("fs", "tp"), P("tp", "fs"), P())
    return jax.shard_map(shards, mesh=mesh, in_specs=in_specs, out_specs=rows, check_vma=False)
```

```python
import jax
import jax.numpy as jnp
from jax import lax
from jax.experimental import pallas as pl
from jax.experimental.pallas import tpu as pltpu
from jax.sharding import PartitionSpec as P

D, F, Q, TOK = 2048, 1408, 704, 512
SENT = 2048
EPS = 1e-06
F32, BF16 = jnp.float32, jnp.bfloat16


def remote_copy(src, dst, send_sem, recv_sem, to):
    return pltpu.make_async_remote_copy(src_ref=src, dst_ref=dst, send_sem=send_sem, recv_sem=recv_sem, device_id=to,
                                        device_id_type=pl.DeviceIdType.MESH)


TOGETHER = {0: (0, 2), 1: (0, 2), 4: (1, 2), 8: (1, 2), 2: (2, 1), 3: (2, 1), 5: (3, 2), 9: (3, 2), 6: (4, 2), 10: (4, 2),
            7: (5, 2), 11: (5, 2)}


def ring_copies(block, half, to_a, to_b, send, recv):
    c = []
    for way in (1, -1):
        c.append((block(0, 0, 0, 0), block(0, 0, way, 0), to_a[way]))
    for way, h in ((1, 0), (-1, 1)):
        c.append((half(-way, 0, 0, 0, h), half(-way, 0, way, 0, h), to_a[way]))
    for way in (1, -1):
        for oa in (0, -1, 1, 2):
            c.append((block(oa, 0, 0, 0), block(oa, 0, 0, way), to_b[way]))
    for way, h in ((1, 0), (-1, 1)):
        for oa in (0, -1, 1, 2):
            c.append((half(oa, -way, 0, 0, h), half(oa, -way, 0, way, h), to_b[way]))
    return [remote_copy(src, dst, send, recv(i), to) for i, (src, dst, to) in enumerate(c)]


def position(offset):
    return (0, 1, 3, 2)[offset % 4]


def kernel(tok_in, pre_ref, gate_in, value_in, down_in, post_ref, out_ref, tok, wg, wv, wd, dd, dz, w, d, t, acc, hid, ps,
           pr, rp, zs, zr, os_, or_, squares, load, ag_r, zw_r, tk_r, pr_r, zr_r, or_r, sent):
    rep, fs, core = lax.axis_index("rep"), lax.axis_index("fs"), lax.axis_index("tp")
    zlo, y, x = fs // 16, (fs // 4) % 4, fs % 4
    z = rep * 2 + zlo

    def device(dz_=0, dy=0, dx=0, other=False):
        zz, yy, xx = (z + dz_ + 4) % 4, (y + dy + 4) % 4, (x + dx + 4) % 4
        return {"rep": zz // 2, "fs": (zz % 2) * 16 + yy * 4 + xx, "tp": 1 - core if other else core}

    to_x = {1: device(dx=1), -1: device(dx=-1)}
    to_y = {1: device(dy=1), -1: device(dy=-1)}
    to_z = {1: device(dz_=1), -1: device(dz_=-1)}
    partner = device(other=True)

    loads = [
        pltpu.make_async_copy(gate_in, wg, load.at[0]),
        pltpu.make_async_copy(value_in, wv, load.at[1]),
        pltpu.make_async_copy(down_in, wd.at[0:64], load.at[2]),
        pltpu.make_async_copy(down_in, wd.at[64:128], load.at[3]),
    ] + [pltpu.make_async_copy(tok_in.at[128 * c:128 * c + 128], tok.at[128 * c:128 * c + 128], load.at[4 + c]) for c in range(4)]
    barrier = pltpu.get_barrier_semaphore()
    for peer in (*to_x.values(), *to_y.values(), *to_z.values(), partner):
        pl.semaphore_signal(barrier, inc=1, device_id=peer, device_id_type=pl.DeviceIdType.MESH)

    for c in loads:
        c.start()

    lanes = lax.broadcasted_iota(jnp.int32, (64, 128), 1)
    low = lanes < 64
    swap = lambda v: pltpu.roll(v, 64, 1)

    loads[0].wait()
    loads[1].wait()
    place = (y * 4 + x) * 64
    for q in (0, 1):
        at = pl.multiple_of(place + (zlo + q) % 2 * (2048 - place), 64)
        g5, v5 = wg[:, 640:768].astype(F32), wv[:, 640:768].astype(F32)
        first = 768 * q
        w[pl.ds(at, 64), 0:640] = wg[:, first:first + 640]
        w[pl.ds(at, 64), 640:1280] = wv[:, first:first + 640]
        mixed = jnp.where(low, g5, swap(v5)) if q == 0 else jnp.where(low, swap(g5), v5)
        w[pl.ds(at, 64), 1280:1408] = mixed.astype(BF16)

    def slot(oy, ox):
        return (y + oy + 4) % 4, (x + ox + 4) % 4

    def gv(first, rows, h):
        def ref(oa, ob, ma, mb):
            yy, xx = slot(ob, oa) if first == "x" else slot(oa, ob)
            at = (yy * 4 + xx) * 64 if first == "x" else 1024 + (xx * 4 + yy) * 64
            return w.at[pl.ds(pl.multiple_of(at + h * rows, rows), rows)]

        return ref

    def dn(first, rows, h):
        def ref(oa, ob, ma, mb):
            oa, ob = position(oa - ma), position(ob - mb)
            at = (0 if first == "x" else 352) + h * rows
            n = (ob * 4 + oa if first == "x" else oa * 4 + ob) * 128
            return d.at[at:at + rows, n:n + 128]

        return ref

    def arrived(ref, sem):
        remote_copy(ref, ref, sem, sem, partner).wait_recv()

    def left(ref, sem):
        remote_copy(ref, ref, sem, sem, partner).wait_send()

    def together(i, kind):
        if i in TOGETHER:
            return TOGETHER[i]
        if kind is gv:
            return 6, 4
        return (6, 1) if i in (12, 16) else (7, 3)

    items = []
    for i, (make, rows, first) in enumerate(((gv, 64, "x"), (gv, 64, "y"), (dn, 352, "x"), (dn, 352, "y"))):
        halves = [make(first, rows // 2, h) for h in (0, 1)]
        half = lambda oa, ob, ma, mb, h, halves=halves: halves[h](oa, ob, ma, mb)
        a, b = (to_x, to_y) if first == "x" else (to_y, to_x)
        sem = lambda n, i=i, make=make: ag_r.at[i, together(n, make)[0]]
        items.append((ring_copies(make(first, rows, 0), half, a, b, sent.at[i // 2], sem), make, i))
    A, B, C, E = items

    def send(item, *which):
        for i in which:
            item[0][i].start()

    def recv(item, which):
        group, blocks = together(which, item[1])
        ref = w.at[0:64 * blocks] if item[1] is gv else d.at[0:352, 0:128 * blocks]
        arrived(ref, ag_r.at[item[2], group])

    def rows_of(ref, at, n):
        return ref.at[pl.ds(pl.multiple_of(at, n), n)]

    zw = []
    for h, way in ((0, 1), (1, -1)):
        dst = rows_of(w, 1024 + (x * 4 + y) * 64 + 32 * h, 32)
        zw.append(remote_copy(w.at[2048 + 32 * h:2080 + 32 * h], dst, sent.at[2], zw_r.at[0], to_z[way]))
    for h, way in ((0, 1), (1, -1)):
        part = pl.ds(352 * h, 352)
        zw.append(remote_copy(dd.at[1 - zlo, part], dz.at[part], sent.at[2], zw_r.at[1], to_z[way]))

    def group_rows(at):
        return t.at[:, pl.ds(at, 128)]

    tok_z, tok_c, tok_f = [], [], []
    for c in range(4):
        r = 128 * c
        mine = 1024 + 512 * (c % 2) + 128 * (c // 2)
        tok_z.append(remote_copy(group_rows(SENT + r), group_rows(mine), sent.at[3], tk_r.at[c % 2], to_z[1 if c < 2 else -1]))
        tok_c.append(remote_copy(group_rows(r), group_rows(512 + r), sent.at[3], tk_r.at[2], partner))
        tok_f.append(remote_copy(group_rows(mine), group_rows(mine + 256), sent.at[3], tk_r.at[3 + c % 2], partner))

    def forward(half):
        arrived(t.at[:, 0:256], tk_r.at[half])
        tok_f[half].start()
        tok_f[half + 2].start()

    def forwarded(half):
        arrived(t.at[:, 0:256], tk_r.at[3 + half])

    gain = pre_ref[...].astype(F32).reshape(1, D)
    low32 = lax.broadcasted_iota(jnp.int32, (32, 128), 1) < 64

    def norm_rows(r):
        v = tok[pl.ds(r, 32), :].astype(F32)
        v = v * lax.rsqrt(jnp.mean(v * v, axis=-1, keepdims=True) + EPS) * gain
        for k in (0, 1):
            straight = pl.multiple_of((zlo + k) % 2 * SENT + r, 32)
            turned = pl.multiple_of((zlo + k + 1) % 2 * SENT + r, 32)
            tiles = [v[:, k * 1024 + 128 * i:k * 1024 + 128 * (i + 1)] for i in range(8)]
            flipped = [swap(s) for s in tiles]
            for i in range(8):
                t[i // 2, pl.ds(straight, 32), 128 * (i % 2):128 * (i % 2 + 1)] = tiles[i].astype(BF16)
            for xx in range(4):
                for p in (0, 1):
                    one, two = 4 * p + xx // 2, 4 * p + 2 + xx // 2
                    if xx % 2 == 0:
                        out = jnp.where(low32, tiles[one], flipped[two])
                    else:
                        out = jnp.where(low32, flipped[one], tiles[two])
                    t[4 + xx, pl.ds(turned, 32), 128 * p:128 * (p + 1)] = out.astype(BF16)

    def norm(c):
        loads[4 + c].wait()
        pl.loop(0, 4)(lambda i: norm_rows(pl.multiple_of(c * 128 + i * 32, 32)))

    def gates(groups, row, count, first):
        for n in range(0, F, 256):
            m = min(256, F - n)
            total = None if first else acc[row:row + count, n:n + m]
            for g in groups:
                part = jnp.dot(t[g, row:row + count, :], w[pl.ds(pl.multiple_of(g * 256, 256), 256), n:n + m],
                               preferred_element_type=F32)
                total = part if total is None else total + part
            acc[row:row + count, n:n + m] = total

    low128 = lax.broadcasted_iota(jnp.int32, (128, 128), 1) < 64

    def hide(row, count):
        def step(i):
            r = pl.multiple_of(row + i * 128, 128)
            for n in range(0, 640, 128):
                g = acc[pl.ds(r, 128), n:n + 128]
                h = g / (1 + jnp.exp(-g)) * acc[pl.ds(r, 128), 640 + n:768 + n]
                hid[pl.ds(r, 128), n:n + 128] = h.astype(BF16)
            m = acc[pl.ds(r, 128), 1280:1408]
            h = m / (1 + jnp.exp(-m)) * swap(m)
            hid[pl.ds(r, 128), 640:768] = jnp.where(low128, h, 0).astype(BF16)

        pl.loop(0, count // 128)(step)

    one, two, last = slice(0, 1), slice(1, 3), slice(3, 4)
    steps = (((one, one),), ((one, two), (two, one)), ((two, two),), ((one, last), (last, one)),
             ((two, last), (last, two), (last, last)))

    def slots_of(parts):
        return [(py, px) for rows, cols in parts for py in range(4)[rows] for px in range(4)[cols]]

    def remote(s, n):
        slots = slots_of(steps[n])
        right = jnp.concatenate([d[:, (py * 4 + px) * 128:(py * 4 + px + 1) * 128] for py, px in slots], axis=1)
        part = jnp.dot(hid[1024 + 512 * s:1536 + 512 * s, :], right, preferred_element_type=F32).astype(BF16)
        for i, (py, px) in enumerate(slots):
            ps[s, py, px] = part[256:512, 128 * i:128 * (i + 1)]
            rp[s, py, px] = part[0:256, 128 * i:128 * (i + 1)]
        for rows, cols in steps[n]:
            remote_copy(ps.at[s, rows, cols], pr.at[s, rows, cols], sent.at[4], pr_r.at[s, n], partner).start()

    def pass_on(s, n):
        slots = slots_of(steps[n])
        arrived(pr.at[s, :, 0] if len(slots) == 4 else d.at[0:256, 0:128 * len(slots)], pr_r.at[s, n])
        for py, px in slots:
            both = (rp[s, py, px].astype(F32) + pr[s, py, px].astype(F32)).astype(BF16)
            zs[s, 0, py, px] = both[0:128]
            zs[s, 1, py, px] = both[128:256]
        for rows, cols in steps[n]:
            for h, way in ((0, -1), (1, 1)):
                remote_copy(zs.at[s, h, rows, cols], zr.at[s, h, rows, cols], sent.at[5], zr_r.at[s, n // 4], to_z[way]).start()

    norm(0)
    pl.semaphore_wait(barrier, 7)
    zw[0].start()
    zw[1].start()
    send(A, 0, 1, 4, 8)
    tok_c[0].start()
    for c in (2, 1, 3):
        norm(c)
        if c == 2:
            tok_z[0].start()
        tok_z[c].start()
        tok_c[c].start()

    loads[2].wait()
    loads[3].wait()
    for i in range(11):
        turned = wd[:, i * 128:(i + 1) * 128].astype(F32).T.astype(BF16)
        at = i * 128
        if i < 5:
            dd[0, at:at + 128] = turned
        elif i == 5:
            dd[0, 640:704] = turned[0:64]
            dd[1, 640:704] = turned[64:128]
        else:
            dd[1, at - 768:at - 640] = turned
    zw[2].start()
    zw[3].start()
    d[Q:768, :] = jnp.zeros((64, D), BF16)

    arrived(w.at[0:64], zw_r.at[0])
    send(B, 0, 1, 4, 8)
    recv(A, 0)
    send(A, 2, 3, 5, 9)
    recv(B, 0)
    send(B, 2, 3, 5, 9)
    recv(A, 4)
    send(A, 6, 10, 12, 16)
    recv(B, 4)
    send(B, 6, 10, 12, 16)
    arrived(t.at[:, 0:512], tk_r.at[2])
    recv(A, 2)
    send(A, 7, 11)
    recv(A, 5)
    send(A, 13, 17)
    recv(B, 2)
    send(B, 7, 11)
    here, near, far = (y, 4 + x), ((y + 1) % 4, (y + 3) % 4, 4 + (x + 1) % 4, 4 + (x + 3) % 4), ((y + 2) % 4, 4 + (x + 2) % 4)
    gates(here, 0, 512, True)
    recv(B, 5)
    send(B, 13, 17)
    forward(0)
    gates(here, 512, 512, True)
    recv(A, 6)
    send(A, 14, 18)
    forwarded(0)
    gates(here, 1024, 512, True)
    recv(B, 6)
    send(B, 14, 18)
    recv(A, 7)
    send(A, 15, 19)
    recv(B, 7)
    send(B, 15, 19)
    forward(1)
    gates(near, 1024, 512, False)

    arrived(dz, zw_r.at[1])
    own_half = (lax.broadcasted_iota(jnp.int32, (Q, 128), 1) < 64) == (zlo == 0)
    d[0:Q, 0:128] = jnp.where(own_half, dd[zlo].astype(F32), dz[...].astype(F32)).astype(BF16)
    send(C, 0, 1)
    send(E, 0, 1)
    send(C, 4, 8)
    send(E, 4, 8)
    gates(here + near, 1536, 256, True)
    forwarded(1)
    gates(here + near, 1792, 256, True)
    recv(A, 12)
    recv(B, 12)
    gates(far, 1024, 512, False)
    hide(1024, 512)
    remote(0, 0)
    recv(C, 0)
    send(C, 2, 3, 5, 9)
    recv(E, 0)
    send(E, 2, 3, 5, 9)
    recv(C, 4)
    send(C, 6, 10, 12, 16)
    recv(E, 4)
    send(E, 6, 10, 12, 16)
    remote(0, 1)
    pass_on(0, 0)
    gates(far, 1536, 512, False)
    pass_on(0, 1)
    hide(1536, 512)
    remote(1, 0)
    remote(1, 1)
    recv(C, 2)
    send(C, 7, 11)
    recv(E, 2)
    send(E, 7, 11)
    pass_on(1, 0)
    pass_on(1, 1)
    recv(C, 5)
    send(C, 13, 17)
    recv(E, 5)
    send(E, 13, 17)
    recv(C, 6)
    send(C, 14, 18)
    recv(E, 6)
    send(E, 14, 18)
    remote(0, 2)
    remote(1, 2)
    gates(near, 0, 512, False)
    pass_on(0, 2)
    pass_on(1, 2)
    recv(C, 7)
    send(C, 15, 19)
    recv(E, 7)
    send(E, 15, 19)
    recv(C, 12)
    recv(E, 12)
    remote(0, 3)
    remote(1, 3)
    gates(near, 512, 512, False)
    pass_on(0, 3)
    pass_on(1, 3)
    recv(C, 13)
    recv(E, 13)
    remote(0, 4)
    remote(1, 4)
    gates(far, 0, 512, False)
    pass_on(0, 4)
    pass_on(1, 4)
    gates(far, 512, 512, False)
    hide(0, 1024)

    for n in range(4):
        cols = slice(512 * n, 512 * (n + 1))
        os_[:, cols] = jnp.dot(hid[512:1024, :], d[:, cols], preferred_element_type=F32).astype(BF16)
        remote_copy(os_.at[:, cols], or_.at[:, cols], sent.at[6], or_r.at[0], partner).start()
    for n in range(4):
        place = slice(512 * (n % 2), 512 * (n % 2 + 1))
        part = jnp.dot(hid[0:512, :], d[:, 512 * n:512 * (n + 1)], preferred_element_type=F32)
        acc[1024 + 512 * (n // 2):1536 + 512 * (n // 2), place] = part
    arrived(or_, or_r.at[0])

    post = post_ref[...].astype(F32).reshape(1, D)
    low16 = lax.broadcasted_iota(jnp.int32, (16, 128), 1) < 64

    def spot(theirs, me):
        o = (theirs - me + 4) % 4
        return o + o // 2 - o // 3 * 2

    spots = [(spot(j // 4, y), spot(j % 4, x)) for j in range(16)]

    early, late = slots_of(sum(steps[:4], ())), slots_of(steps[4])

    def mine(row, py, px):
        return acc.at[pl.ds(pl.multiple_of(1024 + py // 2 * 512 + row, 16), 16), (py % 2 * 4 + px) * 128:(py % 2 * 4 + px + 1) * 128]

    def theirs(row, py, px):
        return or_.at[pl.ds(row, 16), (py * 4 + px) * 128:(py * 4 + px + 1) * 128]

    def places(s, h, i):
        r = pl.multiple_of(i * 16, 16)
        return r, pl.multiple_of((2 * h + s) * 128 + r, 16)

    def prepare(s, h, i):
        r, row = places(s, h, i)
        square = jnp.zeros((16, 128), F32)
        for py, px in early:
            v = mine(row, py, px)[...] + theirs(row, py, px)[...].astype(F32)
            v = (v + zr[s, h, py, px, pl.ds(r, 16), :].astype(F32)).astype(BF16)
            theirs(row, py, px)[...] = v
            square += v.astype(F32) * v.astype(F32)
        for py, px in late:
            mine(row, py, px)[...] += theirs(row, py, px)[...].astype(F32)
        squares[pl.ds(row, 16), :] = square

    def finish(s, h, i):
        r, row = places(s, h, i)
        square = squares[pl.ds(row, 16), :]
        for py, px in late:
            v = (mine(row, py, px)[...] + zr[s, h, py, px, pl.ds(r, 16), :].astype(F32)).astype(BF16)
            theirs(row, py, px)[...] = v
            square += v.astype(F32) * v.astype(F32)
        squares[pl.ds(row, 16), :] = square

    def scales(s, h, i):
        r, row = places(s, h, i)
        mean = jnp.sum(squares[pl.ds(row, 16), :], axis=-1, keepdims=True) * (1 / D)
        squares[pl.ds(row, 16), :] = jnp.broadcast_to(0.5 * lax.rsqrt(mean + EPS), (16, 128))

    def write(s, h, i):
        r, row = places(s, h, i)
        scale = squares[pl.ds(row, 16), :]
        b = []
        for py, px in spots:
            b.append(or_[pl.ds(row, 16), pl.ds(pl.multiple_of((py * 4 + px) * 128, 128), 128)].astype(F32))
        for j in range(16):
            one, two = b[2 * (j % 8)], b[2 * (j % 8) + 1]
            v = jnp.where(low16, one, swap(two)) if j < 8 else jnp.where(low16, swap(one), two)
            cols = slice(128 * j, 128 * (j + 1))
            v = tok[pl.ds(row, 16), cols].astype(F32) + v * scale * post[:, cols]
            out_ref[pl.ds(row, 16), cols] = v.astype(BF16)

    for s in (0, 1):
        arrived(d.at[0:176], zr_r.at[s, 0])
        for h in (0, 1):
            pl.loop(0, 8, unroll=2)(lambda i, s=s, h=h: prepare(s, h, i))
    for s in (0, 1):
        arrived(d.at[0:80], zr_r.at[s, 1])
        for h in (0, 1):
            pl.loop(0, 8, unroll=4)(lambda i, s=s, h=h: finish(s, h, i))
        for h in (0, 1):
            pl.loop(0, 8, unroll=8)(lambda i, s=s, h=h: scales(s, h, i))
        for h in (0, 1):
            pl.loop(0, 8, unroll=2)(lambda i, s=s, h=h: write(s, h, i))

    left(w.at[0:1920], sent.at[0])
    left(w.at[0:960], sent.at[1])
    left(w.at[0:128], sent.at[2])
    left(t.at[:, 0:1536], sent.at[3])
    left(ps, sent.at[4])
    left(zs, sent.at[5])
    left(os_, sent.at[6])


def shards(tokens, pre_gain, gate_weight, value_weight, down_weight, post_gain):
    any_, vmem = pl.BlockSpec(memory_space=pl.ANY), pl.BlockSpec(memory_space=pltpu.VMEM)
    sem = pltpu.SemaphoreType.DMA
    buf = lambda *s, t=BF16: pltpu.VMEM(s, t)
    return pl.pallas_call(
        kernel,
        out_shape=pltpu.VMEM((TOK, D), BF16),
        in_specs=[any_, vmem, any_, any_, any_, vmem],
        out_specs=vmem,
        scratch_shapes=[
            buf(TOK, D), buf(64, F), buf(64, F), buf(128, F), buf(2, Q, 128), buf(Q, 128), buf(2112, F), buf(768, D),
            buf(8, 2560, 256), buf(2048, F, t=F32), buf(2048, 768), *[buf(2, 4, 4, 256, 128)] * 3, *[buf(2, 2, 4, 4, 128, 128)] * 2,
            buf(TOK, D), buf(TOK, D), buf(TOK, 128, t=F32),
            sem((8,)), sem((4, 8)), sem((2,)), sem((5,)), sem((2, 5)), sem((2, 2)), sem((1,)), sem((7,)),
        ],
        compiler_params=pltpu.CompilerParams(collective_id=0, has_side_effects=True, vmem_limit_bytes=61 * 1024 * 1024),
    )(tokens, pre_gain, gate_weight, value_weight, down_weight.T, post_gain)


def solution(mesh):
    rows = P(("rep", "fs", "tp"), None)
    in_specs = (rows, P(), P("fs", "tp"), P("fs", "tp"), P("tp", "fs"), P())
    return jax.shard_map(shards, mesh=mesh, in_specs=in_specs, out_specs=rows, check_vma=False)
```

```python
import jax
import jax.numpy as jnp
from jax import lax
from jax.experimental import pallas as pl
from jax.experimental.pallas import tpu as pltpu
from jax.sharding import PartitionSpec as P

D, F, Q, TOK = 2048, 1408, 704, 512
SENT = 2048
EPS = 1e-06
F32, BF16 = jnp.float32, jnp.bfloat16


def remote_copy(src, dst, send_sem, recv_sem, to):
    return pltpu.make_async_remote_copy(src_ref=src, dst_ref=dst, send_sem=send_sem, recv_sem=recv_sem, device_id=to,
                                        device_id_type=pl.DeviceIdType.MESH)


TOGETHER = {0: (0, 2), 1: (0, 2), 4: (1, 2), 8: (1, 2), 2: (2, 1), 3: (2, 1), 5: (3, 2), 9: (3, 2), 6: (4, 2), 10: (4, 2),
            7: (5, 2), 11: (5, 2)}


def ring_copies(block, half, to_a, to_b, send, recv):
    c = []
    for way in (1, -1):
        c.append((block(0, 0, 0, 0), block(0, 0, way, 0), to_a[way]))
    for way, h in ((1, 0), (-1, 1)):
        c.append((half(-way, 0, 0, 0, h), half(-way, 0, way, 0, h), to_a[way]))
    for way in (1, -1):
        for oa in (0, -1, 1, 2):
            c.append((block(oa, 0, 0, 0), block(oa, 0, 0, way), to_b[way]))
    for way, h in ((1, 0), (-1, 1)):
        for oa in (0, -1, 1, 2):
            c.append((half(oa, -way, 0, 0, h), half(oa, -way, 0, way, h), to_b[way]))
    return [remote_copy(src, dst, send, recv(i), to) for i, (src, dst, to) in enumerate(c)]


def position(offset):
    return (0, 1, 3, 2)[offset % 4]


def kernel(tok_in, pre_ref, gate_in, value_in, down_in, post_ref, out_ref, tok, wg, wv, wd, dd, dz, w, d, t, acc, hid, ps,
           pr, rp, zs, zr, os_, or_, squares, load, ag_r, zw_r, tk_r, pr_r, zr_r, or_r, sent):
    rep, fs, core = lax.axis_index("rep"), lax.axis_index("fs"), lax.axis_index("tp")
    zlo, y, x = fs // 16, (fs // 4) % 4, fs % 4
    z = rep * 2 + zlo

    def device(dz_=0, dy=0, dx=0, other=False):
        zz, yy, xx = (z + dz_ + 4) % 4, (y + dy + 4) % 4, (x + dx + 4) % 4
        return {"rep": zz // 2, "fs": (zz % 2) * 16 + yy * 4 + xx, "tp": 1 - core if other else core}

    to_x = {1: device(dx=1), -1: device(dx=-1)}
    to_y = {1: device(dy=1), -1: device(dy=-1)}
    to_z = {1: device(dz_=1), -1: device(dz_=-1)}
    partner = device(other=True)

    loads = [
        pltpu.make_async_copy(gate_in, wg, load.at[0]),
        pltpu.make_async_copy(value_in, wv, load.at[1]),
        pltpu.make_async_copy(down_in, wd.at[0:64], load.at[2]),
        pltpu.make_async_copy(down_in, wd.at[64:128], load.at[3]),
    ] + [pltpu.make_async_copy(tok_in.at[128 * c:128 * c + 128], tok.at[128 * c:128 * c + 128], load.at[4 + c]) for c in range(4)]
    barrier = pltpu.get_barrier_semaphore()
    for peer in (*to_x.values(), *to_y.values(), *to_z.values(), partner):
        pl.semaphore_signal(barrier, inc=1, device_id=peer, device_id_type=pl.DeviceIdType.MESH)

    for c in loads:
        c.start()

    lanes = lax.broadcasted_iota(jnp.int32, (64, 128), 1)
    low = lanes < 64
    swap = lambda v: pltpu.roll(v, 64, 1)

    loads[0].wait()
    loads[1].wait()
    place = (y * 4 + x) * 64
    for q in (0, 1):
        at = pl.multiple_of(place + (zlo + q) % 2 * (2048 - place), 64)
        g5, v5 = wg[:, 640:768].astype(F32), wv[:, 640:768].astype(F32)
        first = 768 * q
        w[pl.ds(at, 64), 0:640] = wg[:, first:first + 640]
        w[pl.ds(at, 64), 640:1280] = wv[:, first:first + 640]
        mixed = jnp.where(low, g5, swap(v5)) if q == 0 else jnp.where(low, swap(g5), v5)
        w[pl.ds(at, 64), 1280:1408] = mixed.astype(BF16)

    def slot(oy, ox):
        return (y + oy + 4) % 4, (x + ox + 4) % 4

    def gv(first, rows, h):
        def ref(oa, ob, ma, mb):
            yy, xx = slot(ob, oa) if first == "x" else slot(oa, ob)
            at = (yy * 4 + xx) * 64 if first == "x" else 1024 + (xx * 4 + yy) * 64
            return w.at[pl.ds(pl.multiple_of(at + h * rows, rows), rows)]

        return ref

    def dn(first, rows, h):
        def ref(oa, ob, ma, mb):
            oa, ob = position(oa - ma), position(ob - mb)
            at = (0 if first == "x" else 352) + h * rows
            n = (ob * 4 + oa if first == "x" else oa * 4 + ob) * 128
            return d.at[at:at + rows, n:n + 128]

        return ref

    def arrived(ref, sem):
        remote_copy(ref, ref, sem, sem, partner).wait_recv()

    def left(ref, sem):
        remote_copy(ref, ref, sem, sem, partner).wait_send()

    def together(i, kind):
        if i in TOGETHER:
            return TOGETHER[i]
        if kind is gv:
            return 6, 4
        return (6, 1) if i in (12, 16) else (7, 3)

    items = []
    for i, (make, rows, first) in enumerate(((gv, 64, "x"), (gv, 64, "y"), (dn, 352, "x"), (dn, 352, "y"))):
        halves = [make(first, rows // 2, h) for h in (0, 1)]
        half = lambda oa, ob, ma, mb, h, halves=halves: halves[h](oa, ob, ma, mb)
        a, b = (to_x, to_y) if first == "x" else (to_y, to_x)
        sem = lambda n, i=i, make=make: ag_r.at[i, together(n, make)[0]]
        items.append((ring_copies(make(first, rows, 0), half, a, b, sent.at[i // 2], sem), make, i))
    A, B, C, E = items

    def send(item, *which):
        for i in which:
            item[0][i].start()

    def recv(item, which):
        group, blocks = together(which, item[1])
        ref = w.at[0:64 * blocks] if item[1] is gv else d.at[0:352, 0:128 * blocks]
        arrived(ref, ag_r.at[item[2], group])

    def rows_of(ref, at, n):
        return ref.at[pl.ds(pl.multiple_of(at, n), n)]

    zw = []
    for h, way in ((0, 1), (1, -1)):
        dst = rows_of(w, 1024 + (x * 4 + y) * 64 + 32 * h, 32)
        zw.append(remote_copy(w.at[2048 + 32 * h:2080 + 32 * h], dst, sent.at[2], zw_r.at[0], to_z[way]))
    for h, way in ((0, 1), (1, -1)):
        part = pl.ds(352 * h, 352)
        zw.append(remote_copy(dd.at[1 - zlo, part], dz.at[part], sent.at[2], zw_r.at[1], to_z[way]))

    def group_rows(at):
        return t.at[:, pl.ds(at, 128)]

    tok_z, tok_c, tok_f = [], [], []
    for c in range(4):
        r = 128 * c
        mine = 1024 + 512 * (c % 2) + 128 * (c // 2)
        tok_z.append(remote_copy(group_rows(SENT + r), group_rows(mine), sent.at[3], tk_r.at[c % 2], to_z[1 if c < 2 else -1]))
        tok_c.append(remote_copy(group_rows(r), group_rows(512 + r), sent.at[3], tk_r.at[2], partner))
        tok_f.append(remote_copy(group_rows(mine), group_rows(mine + 256), sent.at[3], tk_r.at[3 + c % 2], partner))

    def forward(half):
        arrived(t.at[:, 0:256], tk_r.at[half])
        tok_f[half].start()
        tok_f[half + 2].start()

    def forwarded(half):
        arrived(t.at[:, 0:256], tk_r.at[3 + half])

    gain = pre_ref[...].astype(F32).reshape(1, D)
    low32 = lax.broadcasted_iota(jnp.int32, (32, 128), 1) < 64

    def norm_rows(r):
        v = tok[pl.ds(r, 32), :].astype(F32)
        v = v * lax.rsqrt(jnp.mean(v * v, axis=-1, keepdims=True) + EPS) * gain
        for k in (0, 1):
            straight = pl.multiple_of((zlo + k) % 2 * SENT + r, 32)
            turned = pl.multiple_of((zlo + k + 1) % 2 * SENT + r, 32)
            tiles = [v[:, k * 1024 + 128 * i:k * 1024 + 128 * (i + 1)] for i in range(8)]
            flipped = [swap(s) for s in tiles]
            for i in range(8):
                t[i // 2, pl.ds(straight, 32), 128 * (i % 2):128 * (i % 2 + 1)] = tiles[i].astype(BF16)
            for xx in range(4):
                for p in (0, 1):
                    one, two = 4 * p + xx // 2, 4 * p + 2 + xx // 2
                    if xx % 2 == 0:
                        out = jnp.where(low32, tiles[one], flipped[two])
                    else:
                        out = jnp.where(low32, flipped[one], tiles[two])
                    t[4 + xx, pl.ds(turned, 32), 128 * p:128 * (p + 1)] = out.astype(BF16)

    def norm(c):
        loads[4 + c].wait()
        pl.loop(0, 4)(lambda i: norm_rows(pl.multiple_of(c * 128 + i * 32, 32)))

    def gates(groups, row, count, first):
        for n in range(0, F, 256):
            m = min(256, F - n)
            total = None if first else acc[row:row + count, n:n + m]
            for g in groups:
                part = jnp.dot(t[g, row:row + count, :], w[pl.ds(pl.multiple_of(g * 256, 256), 256), n:n + m],
                               preferred_element_type=F32)
                total = part if total is None else total + part
            acc[row:row + count, n:n + m] = total

    low128 = lax.broadcasted_iota(jnp.int32, (128, 128), 1) < 64

    def hide(row, count):
        def step(i):
            r = pl.multiple_of(row + i * 128, 128)
            for n in range(0, 640, 128):
                g = acc[pl.ds(r, 128), n:n + 128]
                h = g / (1 + jnp.exp(-g)) * acc[pl.ds(r, 128), 640 + n:768 + n]
                hid[pl.ds(r, 128), n:n + 128] = h.astype(BF16)
            m = acc[pl.ds(r, 128), 1280:1408]
            h = m / (1 + jnp.exp(-m)) * swap(m)
            hid[pl.ds(r, 128), 640:768] = jnp.where(low128, h, 0).astype(BF16)

        pl.loop(0, count // 128)(step)

    one, two, last = slice(0, 1), slice(1, 3), slice(3, 4)
    steps = (((one, one),), ((one, two), (two, one)), ((two, two),), ((one, last), (last, one)),
             ((two, last), (last, two), (last, last)))

    def slots_of(parts):
        return [(py, px) for rows, cols in parts for py in range(4)[rows] for px in range(4)[cols]]

    def remote(s, n):
        slots = slots_of(steps[n])
        right = jnp.concatenate([d[:, (py * 4 + px) * 128:(py * 4 + px + 1) * 128] for py, px in slots], axis=1)
        part = jnp.dot(hid[1024 + 512 * s:1536 + 512 * s, :], right, preferred_element_type=F32).astype(BF16)
        for i, (py, px) in enumerate(slots):
            ps[s, py, px] = part[256:512, 128 * i:128 * (i + 1)]
            rp[s, py, px] = part[0:256, 128 * i:128 * (i + 1)]
        for rows, cols in steps[n]:
            remote_copy(ps.at[s, rows, cols], pr.at[s, rows, cols], sent.at[4], pr_r.at[s, n], partner).start()

    def pass_on(s, n):
        slots = slots_of(steps[n])
        arrived(pr.at[s, :, 0] if len(slots) == 4 else d.at[0:256, 0:128 * len(slots)], pr_r.at[s, n])
        for py, px in slots:
            both = (rp[s, py, px].astype(F32) + pr[s, py, px].astype(F32)).astype(BF16)
            zs[s, 0, py, px] = both[0:128]
            zs[s, 1, py, px] = both[128:256]
        for rows, cols in steps[n]:
            for h, way in ((0, -1), (1, 1)):
                remote_copy(zs.at[s, h, rows, cols], zr.at[s, h, rows, cols], sent.at[5], zr_r.at[s, n // 4], to_z[way]).start()

    norm(0)
    pl.semaphore_wait(barrier, 7)
    zw[0].start()
    zw[1].start()
    send(A, 0, 1, 4, 8)
    tok_c[0].start()
    for c in (2, 1, 3):
        norm(c)
        if c == 2:
            tok_z[0].start()
        tok_z[c].start()
        tok_c[c].start()

    loads[2].wait()
    loads[3].wait()
    for i in range(11):
        turned = wd[:, i * 128:(i + 1) * 128].astype(F32).T.astype(BF16)
        at = i * 128
        if i < 5:
            dd[0, at:at + 128] = turned
        elif i == 5:
            dd[0, 640:704] = turned[0:64]
            dd[1, 640:704] = turned[64:128]
        else:
            dd[1, at - 768:at - 640] = turned
    zw[2].start()
    zw[3].start()
    d[Q:768, :] = jnp.zeros((64, D), BF16)

    arrived(w.at[0:64], zw_r.at[0])
    send(B, 0, 1, 4, 8)
    recv(A, 0)
    send(A, 2, 3, 5, 9)
    recv(B, 0)
    send(B, 2, 3, 5, 9)
    recv(A, 4)
    send(A, 6, 10, 12, 16)
    recv(B, 4)
    send(B, 6, 10, 12, 16)
    arrived(t.at[:, 0:512], tk_r.at[2])
    recv(A, 2)
    send(A, 7, 11)
    recv(A, 5)
    send(A, 13, 17)
    recv(B, 2)
    send(B, 7, 11)
    here, near, far = (y, 4 + x), ((y + 1) % 4, (y + 3) % 4, 4 + (x + 1) % 4, 4 + (x + 3) % 4), ((y + 2) % 4, 4 + (x + 2) % 4)
    gates(here, 0, 512, True)
    recv(B, 5)
    send(B, 13, 17)
    forward(0)
    gates(here, 512, 512, True)
    recv(A, 6)
    send(A, 14, 18)
    forwarded(0)
    gates(here, 1024, 512, True)
    recv(B, 6)
    send(B, 14, 18)
    recv(A, 7)
    send(A, 15, 19)
    recv(B, 7)
    send(B, 15, 19)
    forward(1)
    gates(near, 1024, 512, False)

    arrived(dz, zw_r.at[1])
    own_half = (lax.broadcasted_iota(jnp.int32, (Q, 128), 1) < 64) == (zlo == 0)
    d[0:Q, 0:128] = jnp.where(own_half, dd[zlo].astype(F32), dz[...].astype(F32)).astype(BF16)
    send(C, 0, 1)
    send(E, 0, 1)
    send(C, 4, 8)
    send(E, 4, 8)
    gates(here + near, 1536, 256, True)
    forwarded(1)
    gates(here + near, 1792, 256, True)
    recv(A, 12)
    recv(B, 12)
    gates(far, 1024, 512, False)
    hide(1024, 512)
    remote(0, 0)
    recv(C, 0)
    send(C, 2, 3, 5, 9)
    recv(E, 0)
    send(E, 2, 3, 5, 9)
    recv(C, 4)
    send(C, 6, 10, 12, 16)
    recv(E, 4)
    send(E, 6, 10, 12, 16)
    remote(0, 1)
    pass_on(0, 0)
    gates(far, 1536, 512, False)
    pass_on(0, 1)
    hide(1536, 512)
    remote(1, 0)
    remote(1, 1)
    recv(C, 2)
    send(C, 7, 11)
    recv(E, 2)
    send(E, 7, 11)
    pass_on(1, 0)
    pass_on(1, 1)
    recv(C, 5)
    send(C, 13, 17)
    recv(E, 5)
    send(E, 13, 17)
    recv(C, 6)
    send(C, 14, 18)
    recv(E, 6)
    send(E, 14, 18)
    remote(0, 2)
    remote(1, 2)
    gates(near, 0, 512, False)
    pass_on(0, 2)
    pass_on(1, 2)
    recv(C, 7)
    send(C, 15, 19)
    recv(E, 7)
    send(E, 15, 19)
    recv(C, 12)
    recv(E, 12)
    remote(0, 3)
    remote(1, 3)
    gates(near + far, 512, 512, False)
    pass_on(0, 3)
    pass_on(1, 3)
    recv(C, 13)
    recv(E, 13)
    remote(0, 4)
    remote(1, 4)
    gates(far, 0, 512, False)
    pass_on(0, 4)
    pass_on(1, 4)
    hide(0, 1024)

    for n in range(4):
        cols = slice(512 * n, 512 * (n + 1))
        os_[:, cols] = jnp.dot(hid[512:1024, :], d[:, cols], preferred_element_type=F32).astype(BF16)
        remote_copy(os_.at[:, cols], or_.at[:, cols], sent.at[6], or_r.at[0], partner).start()
    for n in range(4):
        place = slice(512 * (n % 2), 512 * (n % 2 + 1))
        part = jnp.dot(hid[0:512, :], d[:, 512 * n:512 * (n + 1)], preferred_element_type=F32)
        acc[1024 + 512 * (n // 2):1536 + 512 * (n // 2), place] = part
    arrived(or_, or_r.at[0])

    post = post_ref[...].astype(F32).reshape(1, D)
    low16 = lax.broadcasted_iota(jnp.int32, (16, 128), 1) < 64

    def spot(theirs, me):
        o = (theirs - me + 4) % 4
        return o + o // 2 - o // 3 * 2

    spots = [(spot(j // 4, y), spot(j % 4, x)) for j in range(16)]

    early, late = slots_of(sum(steps[:4], ())), slots_of(steps[4])

    def mine(row, py, px):
        return acc.at[pl.ds(pl.multiple_of(1024 + py // 2 * 512 + row, 16), 16), (py % 2 * 4 + px) * 128:(py % 2 * 4 + px + 1) * 128]

    def theirs(row, py, px):
        return or_.at[pl.ds(row, 16), (py * 4 + px) * 128:(py * 4 + px + 1) * 128]

    def places(s, h, i):
        r = pl.multiple_of(i * 16, 16)
        return r, pl.multiple_of((2 * h + s) * 128 + r, 16)

    def prepare(s, h, i):
        r, row = places(s, h, i)
        square = jnp.zeros((16, 128), F32)
        for py, px in early:
            v = mine(row, py, px)[...] + theirs(row, py, px)[...].astype(F32)
            v = (v + zr[s, h, py, px, pl.ds(r, 16), :].astype(F32)).astype(BF16)
            theirs(row, py, px)[...] = v
            square += v.astype(F32) * v.astype(F32)
        for py, px in late:
            mine(row, py, px)[...] += theirs(row, py, px)[...].astype(F32)
        squares[pl.ds(row, 16), :] = square

    def finish(s, h, i):
        r, row = places(s, h, i)
        square = squares[pl.ds(row, 16), :]
        for py, px in late:
            v = (mine(row, py, px)[...] + zr[s, h, py, px, pl.ds(r, 16), :].astype(F32)).astype(BF16)
            theirs(row, py, px)[...] = v
            square += v.astype(F32) * v.astype(F32)
        squares[pl.ds(row, 16), :] = square

    def scales(s, h, i):
        r, row = places(s, h, i)
        mean = jnp.sum(squares[pl.ds(row, 16), :], axis=-1, keepdims=True) * (1 / D)
        squares[pl.ds(row, 16), :] = jnp.broadcast_to(0.5 * lax.rsqrt(mean + EPS), (16, 128))

    def write(s, h, i):
        r, row = places(s, h, i)
        scale = squares[pl.ds(row, 16), :]
        b = []
        for py, px in spots:
            b.append(or_[pl.ds(row, 16), pl.ds(pl.multiple_of((py * 4 + px) * 128, 128), 128)].astype(F32))
        for j in range(16):
            one, two = b[2 * (j % 8)], b[2 * (j % 8) + 1]
            v = jnp.where(low16, one, swap(two)) if j < 8 else jnp.where(low16, swap(one), two)
            cols = slice(128 * j, 128 * (j + 1))
            v = tok[pl.ds(row, 16), cols].astype(F32) + v * scale * post[:, cols]
            out_ref[pl.ds(row, 16), cols] = v.astype(BF16)

    for s in (0, 1):
        arrived(d.at[0:176], zr_r.at[s, 0])
        for h in (0, 1):
            pl.loop(0, 8, unroll=4)(lambda i, s=s, h=h: prepare(s, h, i))
    for s in (0, 1):
        arrived(d.at[0:80], zr_r.at[s, 1])
        for h in (0, 1):
            pl.loop(0, 8, unroll=4)(lambda i, s=s, h=h: finish(s, h, i))
        for h in (0, 1):
            pl.loop(0, 8, unroll=8)(lambda i, s=s, h=h: scales(s, h, i))
        for h in (0, 1):
            pl.loop(0, 8, unroll=4)(lambda i, s=s, h=h: write(s, h, i))

    left(w.at[0:1920], sent.at[0])
    left(w.at[0:960], sent.at[1])
    left(w.at[0:128], sent.at[2])
    left(t.at[:, 0:1536], sent.at[3])
    left(ps, sent.at[4])
    left(zs, sent.at[5])
    left(os_, sent.at[6])


def shards(tokens, pre_gain, gate_weight, value_weight, down_weight, post_gain):
    any_, vmem = pl.BlockSpec(memory_space=pl.ANY), pl.BlockSpec(memory_space=pltpu.VMEM)
    sem = pltpu.SemaphoreType.DMA
    buf = lambda *s, t=BF16: pltpu.VMEM(s, t)
    return pl.pallas_call(
        kernel,
        out_shape=pltpu.VMEM((TOK, D), BF16),
        in_specs=[any_, vmem, any_, any_, any_, vmem],
        out_specs=vmem,
        scratch_shapes=[
            buf(TOK, D), buf(64, F), buf(64, F), buf(128, F), buf(2, Q, 128), buf(Q, 128), buf(2112, F), buf(768, D),
            buf(8, 2560, 256), buf(2048, F, t=F32), buf(2048, 768), *[buf(2, 4, 4, 256, 128)] * 3, *[buf(2, 2, 4, 4, 128, 128)] * 2,
            buf(TOK, D), buf(TOK, D), buf(TOK, 128, t=F32),
            sem((8,)), sem((4, 8)), sem((2,)), sem((5,)), sem((2, 5)), sem((2, 2)), sem((1,)), sem((7,)),
        ],
        compiler_params=pltpu.CompilerParams(collective_id=0, has_side_effects=True, vmem_limit_bytes=61 * 1024 * 1024),
    )(tokens, pre_gain, gate_weight, value_weight, down_weight.T, post_gain)


def solution(mesh):
    rows = P(("rep", "fs", "tp"), None)
    in_specs = (rows, P(), P("fs", "tp"), P("fs", "tp"), P("tp", "fs"), P())
    return jax.shard_map(shards, mesh=mesh, in_specs=in_specs, out_specs=rows, check_vma=False)
```

```python
import jax
import jax.numpy as jnp
from jax import lax
from jax.experimental import pallas as pl
from jax.experimental.pallas import tpu as pltpu
from jax.sharding import PartitionSpec as P

D, F, Q, TOK = 2048, 1408, 704, 512
SENT = 2048
EPS = 1e-06
F32, BF16 = jnp.float32, jnp.bfloat16


def remote_copy(src, dst, send_sem, recv_sem, to):
    return pltpu.make_async_remote_copy(src_ref=src, dst_ref=dst, send_sem=send_sem, recv_sem=recv_sem, device_id=to,
                                        device_id_type=pl.DeviceIdType.MESH)


TOGETHER = {0: (0, 2), 1: (0, 2), 4: (1, 2), 8: (1, 2), 2: (2, 1), 3: (2, 1), 5: (3, 2), 9: (3, 2), 6: (4, 2), 10: (4, 2),
            7: (5, 2), 11: (5, 2)}


def ring_copies(block, half, to_a, to_b, send, recv):
    c = []
    for way in (1, -1):
        c.append((block(0, 0, 0, 0), block(0, 0, way, 0), to_a[way]))
    for way, h in ((1, 0), (-1, 1)):
        c.append((half(-way, 0, 0, 0, h), half(-way, 0, way, 0, h), to_a[way]))
    for way in (1, -1):
        for oa in (0, -1, 1, 2):
            c.append((block(oa, 0, 0, 0), block(oa, 0, 0, way), to_b[way]))
    for way, h in ((1, 0), (-1, 1)):
        for oa in (0, -1, 1, 2):
            c.append((half(oa, -way, 0, 0, h), half(oa, -way, 0, way, h), to_b[way]))
    return [remote_copy(src, dst, send, recv(i), to) for i, (src, dst, to) in enumerate(c)]


def position(offset):
    return (0, 1, 3, 2)[offset % 4]


def kernel(tok_in, pre_ref, gate_in, value_in, down_in, post_ref, out_ref, tok, wg, wv, wd, dd, dz, w, d, t, acc, hid, ps,
           pr, rp, zs, zr, os_, or_, squares, load, ag_r, zw_r, tk_r, pr_r, zr_r, or_r, sent):
    rep, fs, core = lax.axis_index("rep"), lax.axis_index("fs"), lax.axis_index("tp")
    zlo, y, x = fs // 16, (fs // 4) % 4, fs % 4
    z = rep * 2 + zlo

    def device(dz_=0, dy=0, dx=0, other=False):
        zz, yy, xx = (z + dz_ + 4) % 4, (y + dy + 4) % 4, (x + dx + 4) % 4
        return {"rep": zz // 2, "fs": (zz % 2) * 16 + yy * 4 + xx, "tp": 1 - core if other else core}

    to_x = {1: device(dx=1), -1: device(dx=-1)}
    to_y = {1: device(dy=1), -1: device(dy=-1)}
    to_z = {1: device(dz_=1), -1: device(dz_=-1)}
    partner = device(other=True)

    loads = [
        pltpu.make_async_copy(gate_in, wg, load.at[0]),
        pltpu.make_async_copy(value_in, wv, load.at[1]),
        pltpu.make_async_copy(down_in, wd.at[0:64], load.at[2]),
        pltpu.make_async_copy(down_in, wd.at[64:128], load.at[3]),
    ] + [pltpu.make_async_copy(tok_in.at[128 * c:128 * c + 128], tok.at[128 * c:128 * c + 128], load.at[4 + c]) for c in range(4)]
    barrier = pltpu.get_barrier_semaphore()
    for peer in (*to_x.values(), *to_y.values(), *to_z.values(), partner):
        pl.semaphore_signal(barrier, inc=1, device_id=peer, device_id_type=pl.DeviceIdType.MESH)

    for c in loads:
        c.start()

    lanes = lax.broadcasted_iota(jnp.int32, (64, 128), 1)
    low = lanes < 64
    swap = lambda v: pltpu.roll(v, 64, 1)

    loads[0].wait()
    loads[1].wait()
    place = (y * 4 + x) * 64
    for q in (0, 1):
        at = pl.multiple_of(place + (zlo + q) % 2 * (2048 - place), 64)
        g5, v5 = wg[:, 640:768].astype(F32), wv[:, 640:768].astype(F32)
        first = 768 * q
        w[pl.ds(at, 64), 0:640] = wg[:, first:first + 640]
        w[pl.ds(at, 64), 640:1280] = wv[:, first:first + 640]
        mixed = jnp.where(low, g5, swap(v5)) if q == 0 else jnp.where(low, swap(g5), v5)
        w[pl.ds(at, 64), 1280:1408] = mixed.astype(BF16)

    def slot(oy, ox):
        return (y + oy + 4) % 4, (x + ox + 4) % 4

    def gv(first, rows, h):
        def ref(oa, ob, ma, mb):
            yy, xx = slot(ob, oa) if first == "x" else slot(oa, ob)
            at = (yy * 4 + xx) * 64 if first == "x" else 1024 + (xx * 4 + yy) * 64
            return w.at[pl.ds(pl.multiple_of(at + h * rows, rows), rows)]

        return ref

    def dn(first, rows, h):
        def ref(oa, ob, ma, mb):
            oa, ob = position(oa - ma), position(ob - mb)
            at = (0 if first == "x" else 352) + h * rows
            n = (ob * 4 + oa if first == "x" else oa * 4 + ob) * 128
            return d.at[at:at + rows, n:n + 128]

        return ref

    def arrived(ref, sem):
        remote_copy(ref, ref, sem, sem, partner).wait_recv()

    def left(ref, sem):
        remote_copy(ref, ref, sem, sem, partner).wait_send()

    def together(i, kind):
        if i in TOGETHER:
            return TOGETHER[i]
        if kind is gv:
            return 6, 4
        return (6, 1) if i in (12, 16) else (7, 3)

    items = []
    for i, (make, rows, first) in enumerate(((gv, 64, "x"), (gv, 64, "y"), (dn, 352, "x"), (dn, 352, "y"))):
        halves = [make(first, rows // 2, h) for h in (0, 1)]
        half = lambda oa, ob, ma, mb, h, halves=halves: halves[h](oa, ob, ma, mb)
        a, b = (to_x, to_y) if first == "x" else (to_y, to_x)
        sem = lambda n, i=i, make=make: ag_r.at[i, together(n, make)[0]]
        items.append((ring_copies(make(first, rows, 0), half, a, b, sent.at[i // 2], sem), make, i))
    A, B, C, E = items

    def send(item, *which):
        for i in which:
            item[0][i].start()

    def recv(item, which):
        group, blocks = together(which, item[1])
        ref = w.at[0:64 * blocks] if item[1] is gv else d.at[0:352, 0:128 * blocks]
        arrived(ref, ag_r.at[item[2], group])

    def rows_of(ref, at, n):
        return ref.at[pl.ds(pl.multiple_of(at, n), n)]

    zw = []
    for h, way in ((0, 1), (1, -1)):
        dst = rows_of(w, 1024 + (x * 4 + y) * 64 + 32 * h, 32)
        zw.append(remote_copy(w.at[2048 + 32 * h:2080 + 32 * h], dst, sent.at[2], zw_r.at[0], to_z[way]))
    for h, way in ((0, 1), (1, -1)):
        part = pl.ds(352 * h, 352)
        zw.append(remote_copy(dd.at[1 - zlo, part], dz.at[part], sent.at[2], zw_r.at[1], to_z[way]))

    def group_rows(at):
        return t.at[:, pl.ds(at, 128)]

    tok_z, tok_c, tok_f = [], [], []
    for c in range(4):
        r = 128 * c
        mine = 1024 + 512 * (c % 2) + 128 * (c // 2)
        tok_z.append(remote_copy(group_rows(SENT + r), group_rows(mine), sent.at[3], tk_r.at[c % 2], to_z[1 if c < 2 else -1]))
        tok_c.append(remote_copy(group_rows(r), group_rows(512 + r), sent.at[3], tk_r.at[2], partner))
        tok_f.append(remote_copy(group_rows(mine), group_rows(mine + 256), sent.at[3], tk_r.at[3 + c % 2], partner))

    def forward(half):
        arrived(t.at[:, 0:256], tk_r.at[half])
        tok_f[half].start()
        tok_f[half + 2].start()

    def forwarded(half):
        arrived(t.at[:, 0:256], tk_r.at[3 + half])

    gain = pre_ref[...].astype(F32).reshape(1, D)
    low32 = lax.broadcasted_iota(jnp.int32, (32, 128), 1) < 64

    def norm_rows(r):
        v = tok[pl.ds(r, 32), :].astype(F32)
        v = v * lax.rsqrt(jnp.mean(v * v, axis=-1, keepdims=True) + EPS) * gain
        for k in (0, 1):
            straight = pl.multiple_of((zlo + k) % 2 * SENT + r, 32)
            turned = pl.multiple_of((zlo + k + 1) % 2 * SENT + r, 32)
            tiles = [v[:, k * 1024 + 128 * i:k * 1024 + 128 * (i + 1)] for i in range(8)]
            flipped = [swap(s) for s in tiles]
            for i in range(8):
                t[i // 2, pl.ds(straight, 32), 128 * (i % 2):128 * (i % 2 + 1)] = tiles[i].astype(BF16)
            for xx in range(4):
                for p in (0, 1):
                    one, two = 4 * p + xx // 2, 4 * p + 2 + xx // 2
                    if xx % 2 == 0:
                        out = jnp.where(low32, tiles[one], flipped[two])
                    else:
                        out = jnp.where(low32, flipped[one], tiles[two])
                    t[4 + xx, pl.ds(turned, 32), 128 * p:128 * (p + 1)] = out.astype(BF16)

    def norm(c):
        loads[4 + c].wait()
        pl.loop(0, 4)(lambda i: norm_rows(pl.multiple_of(c * 128 + i * 32, 32)))

    def gates(groups, row, count, first):
        for n in range(0, F, 256):
            m = min(256, F - n)
            total = None if first else acc[row:row + count, n:n + m]
            for g in groups:
                part = jnp.dot(t[g, row:row + count, :], w[pl.ds(pl.multiple_of(g * 256, 256), 256), n:n + m],
                               preferred_element_type=F32)
                total = part if total is None else total + part
            acc[row:row + count, n:n + m] = total

    low128 = lax.broadcasted_iota(jnp.int32, (128, 128), 1) < 64

    def hide(row, count):
        def step(i):
            r = pl.multiple_of(row + i * 128, 128)
            for n in range(0, 640, 128):
                g = acc[pl.ds(r, 128), n:n + 128]
                h = g / (1 + jnp.exp(-g)) * acc[pl.ds(r, 128), 640 + n:768 + n]
                hid[pl.ds(r, 128), n:n + 128] = h.astype(BF16)
            m = acc[pl.ds(r, 128), 1280:1408]
            h = m / (1 + jnp.exp(-m)) * swap(m)
            hid[pl.ds(r, 128), 640:768] = jnp.where(low128, h, 0).astype(BF16)

        pl.loop(0, count // 128)(step)

    one, two, last = slice(0, 1), slice(1, 3), slice(3, 4)
    steps = (((one, one),), ((one, two), (two, one)), ((two, two),), ((one, last), (last, one)),
             ((two, last), (last, two), (last, last)))

    def slots_of(parts):
        return [(py, px) for rows, cols in parts for py in range(4)[rows] for px in range(4)[cols]]

    def remote(s, n):
        slots = slots_of(steps[n])
        right = jnp.concatenate([d[:, (py * 4 + px) * 128:(py * 4 + px + 1) * 128] for py, px in slots], axis=1)
        part = jnp.dot(hid[1024 + 512 * s:1536 + 512 * s, :], right, preferred_element_type=F32).astype(BF16)
        for i, (py, px) in enumerate(slots):
            ps[s, py, px] = part[256:512, 128 * i:128 * (i + 1)]
        for rows, cols in steps[n]:
            remote_copy(ps.at[s, rows, cols], pr.at[s, rows, cols], sent.at[4], pr_r.at[s, n], partner).start()
        for i, (py, px) in enumerate(slots):
            rp[s, py, px] = part[0:256, 128 * i:128 * (i + 1)]

    def pass_on(s, n):
        slots = slots_of(steps[n])
        arrived(pr.at[s, :, 0] if len(slots) == 4 else d.at[0:256, 0:128 * len(slots)], pr_r.at[s, n])
        for py, px in slots:
            both = (rp[s, py, px].astype(F32) + pr[s, py, px].astype(F32)).astype(BF16)
            zs[s, 0, py, px] = both[0:128]
            zs[s, 1, py, px] = both[128:256]
        for rows, cols in steps[n]:
            for h, way in ((0, -1), (1, 1)):
                remote_copy(zs.at[s, h, rows, cols], zr.at[s, h, rows, cols], sent.at[5], zr_r.at[s, n // 4], to_z[way]).start()

    norm(0)
    pl.semaphore_wait(barrier, 7)
    zw[0].start()
    zw[1].start()
    send(A, 0, 1, 4, 8)
    tok_c[0].start()
    for c in (2, 1, 3):
        norm(c)
        if c == 2:
            tok_z[0].start()
        tok_z[c].start()
        tok_c[c].start()

    loads[2].wait()
    loads[3].wait()
    for i in range(11):
        turned = wd[:, i * 128:(i + 1) * 128].astype(F32).T.astype(BF16)
        at = i * 128
        if i < 5:
            dd[0, at:at + 128] = turned
        elif i == 5:
            dd[0, 640:704] = turned[0:64]
            dd[1, 640:704] = turned[64:128]
        else:
            dd[1, at - 768:at - 640] = turned
    zw[2].start()
    zw[3].start()
    d[Q:768, :] = jnp.zeros((64, D), BF16)

    arrived(w.at[0:64], zw_r.at[0])
    send(B, 0, 1, 4, 8)
    recv(A, 0)
    send(A, 2, 3, 5, 9)
    recv(B, 0)
    send(B, 2, 3, 5, 9)
    recv(A, 4)
    send(A, 6, 10, 12, 16)
    recv(B, 4)
    send(B, 6, 10, 12, 16)
    arrived(t.at[:, 0:512], tk_r.at[2])
    recv(A, 2)
    send(A, 7, 11)
    recv(A, 5)
    send(A, 13, 17)
    recv(B, 2)
    send(B, 7, 11)
    here, near, far = (y, 4 + x), ((y + 1) % 4, (y + 3) % 4, 4 + (x + 1) % 4, 4 + (x + 3) % 4), ((y + 2) % 4, 4 + (x + 2) % 4)
    gates(here, 0, 512, True)
    recv(B, 5)
    send(B, 13, 17)
    forward(0)
    gates(here, 512, 512, True)
    recv(A, 6)
    send(A, 14, 18)
    forwarded(0)
    gates(here, 1024, 512, True)
    recv(B, 6)
    send(B, 14, 18)
    recv(A, 7)
    send(A, 15, 19)
    recv(B, 7)
    send(B, 15, 19)
    forward(1)
    gates(near, 1024, 512, False)

    arrived(dz, zw_r.at[1])
    own_half = (lax.broadcasted_iota(jnp.int32, (Q, 128), 1) < 64) == (zlo == 0)
    d[0:Q, 0:128] = jnp.where(own_half, dd[zlo].astype(F32), dz[...].astype(F32)).astype(BF16)
    send(C, 0, 1)
    send(E, 0, 1)
    send(C, 4, 8)
    send(E, 4, 8)
    gates(here + near, 1536, 256, True)
    forwarded(1)
    gates(here + near, 1792, 256, True)
    recv(A, 12)
    recv(B, 12)
    gates(far, 1024, 512, False)
    hide(1024, 512)
    remote(0, 0)
    recv(C, 0)
    send(C, 2, 3, 5, 9)
    recv(E, 0)
    send(E, 2, 3, 5, 9)
    recv(C, 4)
    send(C, 6, 10, 12, 16)
    recv(E, 4)
    send(E, 6, 10, 12, 16)
    remote(0, 1)
    pass_on(0, 0)
    gates(far, 1536, 512, False)
    pass_on(0, 1)
    hide(1536, 512)
    remote(1, 0)
    remote(1, 1)
    recv(C, 2)
    send(C, 7, 11)
    recv(E, 2)
    send(E, 7, 11)
    pass_on(1, 0)
    pass_on(1, 1)
    recv(C, 5)
    send(C, 13, 17)
    recv(E, 5)
    send(E, 13, 17)
    recv(C, 6)
    send(C, 14, 18)
    recv(E, 6)
    send(E, 14, 18)
    remote(0, 2)
    remote(1, 2)
    gates(near, 0, 512, False)
    pass_on(0, 2)
    pass_on(1, 2)
    recv(C, 7)
    send(C, 15, 19)
    recv(E, 7)
    send(E, 15, 19)
    recv(C, 12)
    recv(E, 12)
    remote(0, 3)
    remote(1, 3)
    gates(near + far, 512, 512, False)
    pass_on(0, 3)
    pass_on(1, 3)
    recv(C, 13)
    recv(E, 13)
    remote(0, 4)
    remote(1, 4)
    gates(far, 0, 512, False)
    pass_on(0, 4)
    pass_on(1, 4)
    hide(0, 1024)

    for n in range(4):
        cols = slice(512 * n, 512 * (n + 1))
        os_[:, cols] = jnp.dot(hid[512:1024, :], d[:, cols], preferred_element_type=F32).astype(BF16)
        remote_copy(os_.at[:, cols], or_.at[:, cols], sent.at[6], or_r.at[0], partner).start()
    for n in range(4):
        place = slice(512 * (n % 2), 512 * (n % 2 + 1))
        part = jnp.dot(hid[0:512, :], d[:, 512 * n:512 * (n + 1)], preferred_element_type=F32)
        acc[1024 + 512 * (n // 2):1536 + 512 * (n // 2), place] = part
    arrived(or_, or_r.at[0])

    post = post_ref[...].astype(F32).reshape(1, D)
    low16 = lax.broadcasted_iota(jnp.int32, (16, 128), 1) < 64

    def spot(theirs, me):
        o = (theirs - me + 4) % 4
        return o + o // 2 - o // 3 * 2

    spots = [(spot(j // 4, y), spot(j % 4, x)) for j in range(16)]

    early, late = slots_of(sum(steps[:4], ())), slots_of(steps[4])

    def mine(row, py, px):
        return acc.at[pl.ds(pl.multiple_of(1024 + py // 2 * 512 + row, 16), 16), (py % 2 * 4 + px) * 128:(py % 2 * 4 + px + 1) * 128]

    def theirs(row, py, px):
        return or_.at[pl.ds(row, 16), (py * 4 + px) * 128:(py * 4 + px + 1) * 128]

    def places(s, h, i):
        r = pl.multiple_of(i * 16, 16)
        return r, pl.multiple_of((2 * h + s) * 128 + r, 16)

    def prepare(s, h, i):
        r, row = places(s, h, i)
        square = jnp.zeros((16, 128), F32)
        for py, px in early:
            v = mine(row, py, px)[...] + theirs(row, py, px)[...].astype(F32)
            v = (v + zr[s, h, py, px, pl.ds(r, 16), :].astype(F32)).astype(BF16)
            theirs(row, py, px)[...] = v
            square += v.astype(F32) * v.astype(F32)
        for py, px in late:
            mine(row, py, px)[...] += theirs(row, py, px)[...].astype(F32)
        squares[pl.ds(row, 16), :] = square

    def finish(s, h, i):
        r, row = places(s, h, i)
        square = squares[pl.ds(row, 16), :]
        for py, px in late:
            v = (mine(row, py, px)[...] + zr[s, h, py, px, pl.ds(r, 16), :].astype(F32)).astype(BF16)
            theirs(row, py, px)[...] = v
            square += v.astype(F32) * v.astype(F32)
        squares[pl.ds(row, 16), :] = square

    def scales(s, h, i):
        r, row = places(s, h, i)
        mean = jnp.sum(squares[pl.ds(row, 16), :], axis=-1, keepdims=True) * (1 / D)
        squares[pl.ds(row, 16), :] = jnp.broadcast_to(0.5 * lax.rsqrt(mean + EPS), (16, 128))

    def write(s, h, i):
        r, row = places(s, h, i)
        scale = squares[pl.ds(row, 16), :]
        b = []
        for py, px in spots:
            b.append(or_[pl.ds(row, 16), pl.ds(pl.multiple_of((py * 4 + px) * 128, 128), 128)].astype(F32))
        for j in range(16):
            one, two = b[2 * (j % 8)], b[2 * (j % 8) + 1]
            v = jnp.where(low16, one, swap(two)) if j < 8 else jnp.where(low16, swap(one), two)
            cols = slice(128 * j, 128 * (j + 1))
            v = tok[pl.ds(row, 16), cols].astype(F32) + v * scale * post[:, cols]
            out_ref[pl.ds(row, 16), cols] = v.astype(BF16)

    for s in (0, 1):
        arrived(d.at[0:176], zr_r.at[s, 0])
        for h in (0, 1):
            pl.loop(0, 8, unroll=8)(lambda i, s=s, h=h: prepare(s, h, i))
    for s in (0, 1):
        arrived(d.at[0:80], zr_r.at[s, 1])
        for h in (0, 1):
            pl.loop(0, 8, unroll=4)(lambda i, s=s, h=h: finish(s, h, i))
        for h in (0, 1):
            pl.loop(0, 8, unroll=8)(lambda i, s=s, h=h: scales(s, h, i))
        for h in (0, 1):
            pl.loop(0, 8, unroll=8)(lambda i, s=s, h=h: write(s, h, i))

    left(w.at[0:1920], sent.at[0])
    left(w.at[0:960], sent.at[1])
    left(w.at[0:128], sent.at[2])
    left(t.at[:, 0:1536], sent.at[3])
    left(ps, sent.at[4])
    left(zs, sent.at[5])
    left(os_, sent.at[6])


def shards(tokens, pre_gain, gate_weight, value_weight, down_weight, post_gain):
    any_, vmem = pl.BlockSpec(memory_space=pl.ANY), pl.BlockSpec(memory_space=pltpu.VMEM)
    sem = pltpu.SemaphoreType.DMA
    buf = lambda *s, t=BF16: pltpu.VMEM(s, t)
    return pl.pallas_call(
        kernel,
        out_shape=pltpu.VMEM((TOK, D), BF16),
        in_specs=[any_, vmem, any_, any_, any_, vmem],
        out_specs=vmem,
        scratch_shapes=[
            buf(TOK, D), buf(64, F), buf(64, F), buf(128, F), buf(2, Q, 128), buf(Q, 128), buf(2112, F), buf(768, D),
            buf(8, 2560, 256), buf(2048, F, t=F32), buf(2048, 768), *[buf(2, 4, 4, 256, 128)] * 3, *[buf(2, 2, 4, 4, 128, 128)] * 2,
            buf(TOK, D), buf(TOK, D), buf(TOK, 128, t=F32),
            sem((8,)), sem((4, 8)), sem((2,)), sem((5,)), sem((2, 5)), sem((2, 2)), sem((1,)), sem((7,)),
        ],
        compiler_params=pltpu.CompilerParams(collective_id=0, has_side_effects=True, vmem_limit_bytes=61 * 1024 * 1024),
    )(tokens, pre_gain, gate_weight, value_weight, down_weight.T, post_gain)


def solution(mesh):
    rows = P(("rep", "fs", "tp"), None)
    in_specs = (rows, P(), P("fs", "tp"), P("fs", "tp"), P("tp", "fs"), P())
    return jax.shard_map(shards, mesh=mesh, in_specs=in_specs, out_specs=rows, check_vma=False)
```
